128 devices in a mesh: sp: 16 (over z, y), tp: 8 (over x, core).
Axes of the slice: x: 4, y: 4, z: 4, core: 2. Of those that a mesh axis runs over, the one named last changes fastest.
Arguments:
- latent: bfloat16 [2048, 4096], P(('sp', 'tp')), may hold values from -8 to 8
- context: bfloat16 [512, 4096], P('sp'), may hold values from -6 to 6
- condition: float32 [4096], P('sp'), may hold values from -6 to 6
- context_condition: float32 [4096], P('sp'), may hold values from -6 to 6
- shift_weight: bfloat16 [4096, 4096], P('sp', 'tp'), may hold values from -0.09375 to 0.09375
- scale_weight: bfloat16 [4096, 4096], P('sp', 'tp'), may hold values from -0.09375 to 0.09375
- gate_weight: bfloat16 [4096, 4096], P('sp', 'tp'), may hold values from -0.09375 to 0.09375
- norm_gain: float32 [4096], replicated, may hold values from 0.1 to 1.9
- decay_down: bfloat16 [4096, 128], replicated, may hold values from -0.09375 to 0.09375
- decay_up: bfloat16 [128, 4096], P(None, 'tp'), may hold values from -0.5 to 0.5
- rate_down: bfloat16 [4096, 128], replicated, may hold values from -0.09375 to 0.09375
- rate_up: bfloat16 [128, 4096], P(None, 'tp'), may hold values from -0.5 to 0.5
- head_bias: float32 [2, 4096], P(None, 'tp'), may hold values from -12 to 1
- query_weight: bfloat16 [4096, 4096], P(None, 'tp'), may hold values from -0.09375 to 0.09375
- key_weight: bfloat16 [4096, 4096], P(None, 'tp'), may hold values from -0.09375 to 0.09375
- value_weight: bfloat16 [4096, 4096], P(None, 'tp'), may hold values from -0.09375 to 0.09375
- branch_weight: bfloat16 [4096, 4096], P(None, 'tp'), may hold values from -0.09375 to 0.09375
- group_gain: float32 [4096], P('tp'), may hold values from 0.1 to 1.9
- out_weight: bfloat16 [4096, 4096], P('tp'), may hold values from -0.09375 to 0.09375
Outputs:
- updated: bfloat16 [2048, 4096], P(('sp', 'tp'))
The draws below stay inside these ranges and needn't reach their ends.
All inputs are finite; a program needn't handle non-finite values.
Results may differ from the reference program's by a relative error of at most 0.017.
Values may be sent and summed in bfloat16 or wider, within the bound.
A program may use at most 128 MiB of HBM per device.

```python
import math
import jax
import jax.numpy as jnp
from jax import lax

D = 4096
HEAD_DIM = 64
RANK = 128
TOKENS = 2048
CONTEXT = 512
N_TP = 8


def draw_latent(key, part):
    base_key = jax.random.fold_in(key, 11)
    shared = jax.random.normal(jax.random.fold_in(base_key, 2), (TOKENS // 64, 1, D), jnp.float32)
    shared = jnp.broadcast_to(shared, (TOKENS // 64, 64, D)).reshape(TOKENS, D)
    noise = jax.random.normal(jax.random.fold_in(base_key, 1), (TOKENS, D), jnp.float32)
    value = noise + 0.8 * shared
    return jnp.clip(value, -8.0, 8.0).astype(jnp.bfloat16)


def draw_head_bias(key, part):
    base_key = jax.random.fold_in(key, 23)
    heads = D // HEAD_DIM
    share = 0.5
    decay_low_end = -12.0
    decay_high_end = -10.0
    rate_low_end = -9.0
    rate_high_end = -7.0
    slow_heads = jax.random.bernoulli(jax.random.fold_in(base_key, 1), share, (heads,))
    slow = jnp.repeat(slow_heads, HEAD_DIM)
    decay_fast = jax.random.uniform(jax.random.fold_in(base_key, 2), (D,), jnp.float32, minval=-4.5, maxval=-2.5)
    decay_slow = jax.random.uniform(jax.random.fold_in(base_key, 3), (D,), jnp.float32, minval=decay_low_end, maxval=decay_high_end)
    rate_fast = jax.random.uniform(jax.random.fold_in(base_key, 4), (D,), jnp.float32, minval=-1.0, maxval=1.0)
    rate_slow = jax.random.uniform(jax.random.fold_in(base_key, 5), (D,), jnp.float32, minval=rate_low_end, maxval=rate_high_end)
    decay_row = jnp.where(slow, decay_slow, decay_fast)
    rate_row = jnp.where(slow, rate_slow, rate_fast)
    return jnp.stack([decay_row, rate_row]).astype(jnp.float32)


def levels(stream_key, extent, pieces, low, largest):
    factor_of, own = 1.0, jax.random.fold_in(stream_key, 6)
    for axis_at, blocks in pieces:
        heights = jnp.exp(jax.random.uniform(jax.random.fold_in(own, axis_at), (blocks,), jnp.float32, low / len(pieces), largest / len(pieces)))
        factor_of = factor_of * jnp.repeat(heights, extent[axis_at] // blocks).reshape([-1 if axis == axis_at else 1 for axis in range(len(extent))])
    return factor_of


def centred(own_key, dims, scale, most, pieces=(), dtype=jnp.bfloat16):
    level = levels(own_key, dims, pieces, -0.22, 0.18) if pieces else 1.0
    values = jax.random.normal(own_key, dims, jnp.float32) * scale * level
    return jnp.minimum(jnp.maximum(values, -most), most).astype(dtype)


def setup_inputs(seed: int = 0) -> dict:
    arg_keys = jax.random.split(jax.random.key(seed), 20)
    return {
        "latent": draw_latent(jax.random.fold_in(arg_keys[19], 71), 0),
        "context": centred(arg_keys[1], (CONTEXT, D), 1.0, 6.0, ((0, 16),)),
        "condition": centred(arg_keys[2], (D,), 1.5, 6.0, ((0, 16),), jnp.float32),
        "context_condition": centred(arg_keys[3], (D,), 1.5, 6.0, ((0, 16),), jnp.float32),
        "shift_weight": centred(arg_keys[4], (D, D), D ** -0.5, 0.09375, ((0, 16), (1, 8))),
        "scale_weight": centred(arg_keys[5], (D, D), D ** -0.5, 0.09375, ((0, 16), (1, 8))),
        "gate_weight": centred(arg_keys[6], (D, D), D ** -0.5, 0.09375, ((0, 16), (1, 8))),
        "norm_gain": jnp.clip(1.0 + 0.18 * jax.random.normal(arg_keys[7], (D,), jnp.float32), 0.1, 1.9),
        "decay_down": centred(arg_keys[8], (D, RANK), D ** -0.5, 0.09375),
        "decay_up": centred(arg_keys[9], (RANK, D), RANK ** -0.5, 0.5, ((1, 8),)),
        "rate_down": centred(arg_keys[10], (D, RANK), D ** -0.5, 0.09375),
        "rate_up": centred(arg_keys[11], (RANK, D), RANK ** -0.5, 0.5, ((1, 8),)),
        "head_bias": draw_head_bias(jax.random.fold_in(arg_keys[19], 71), 0),
        "query_weight": centred(arg_keys[13], (D, D), D ** -0.5, 0.09375, ((1, 8),)),
        "key_weight": centred(arg_keys[14], (D, D), D ** -0.5, 0.09375, ((1, 8),)),
        "value_weight": centred(arg_keys[15], (D, D), D ** -0.5, 0.09375, ((1, 8),)),
        "branch_weight": centred(arg_keys[16], (D, D), D ** -0.5, 0.09375, ((1, 8),)),
        "group_gain": jnp.clip(1.0 + 0.18 * jax.random.normal(arg_keys[17], (D,), jnp.float32), 0.1, 1.9),
        "out_weight": centred(arg_keys[18], (D, D), D ** -0.5, 0.09375, ((0, 8),)),
    }


NORM_EPS = 1e-06
GROUP_EPS = 0.00064
DECAY_TOP = math.exp(-0.5)
highest = lax.Precision.HIGHEST

def modulated(rows, gain, scale, shift):
    values = rows.astype(jnp.float32)
    inverse = lax.rsqrt(lax.optimization_barrier(jnp.mean(values * values, axis=-1, keepdims=True)) + NORM_EPS)
    return (values * inverse * gain * (1.0 + scale) + shift).astype(jnp.bfloat16)

def features(normed, key_weight, value_weight, decay_down, decay_up, rate_down, rate_up):
    keys = jnp.dot(normed, key_weight, preferred_element_type=jnp.float32).astype(jnp.bfloat16)
    values = jnp.dot(normed, value_weight, preferred_element_type=jnp.float32).astype(jnp.bfloat16)
    decay_low = jnp.tanh(jnp.dot(normed, decay_down, preferred_element_type=jnp.float32)).astype(jnp.bfloat16)
    rate_low = jnp.dot(normed, rate_down, preferred_element_type=jnp.float32).astype(jnp.bfloat16)
    decay_pre = jnp.dot(decay_low, decay_up, preferred_element_type=jnp.float32).astype(jnp.bfloat16)
    rate_pre = jnp.dot(rate_low, rate_up, preferred_element_type=jnp.float32).astype(jnp.bfloat16)
    return (keys, values, decay_pre, rate_pre)

def chain_inputs(keys, values, decay_pre, rate_pre, head_bias):
    rows = keys.shape[0]
    log_decay = -DECAY_TOP * jax.nn.sigmoid(head_bias[0] + decay_pre.astype(jnp.float32))
    rate = jax.nn.sigmoid(head_bias[1] + rate_pre.astype(jnp.float32))
    key_heads = keys.astype(jnp.float32).reshape(rows, -1, HEAD_DIM)
    unit = key_heads * lax.rsqrt(lax.optimization_barrier(jnp.sum(key_heads * key_heads, axis=-1, keepdims=True)) + 1.0)
    value_heads = values.astype(jnp.float32).reshape(rows, -1, HEAD_DIM)
    write = unit * rate.reshape(rows, -1, HEAD_DIM)
    decay = jnp.exp(log_decay).reshape(rows, -1, HEAD_DIM)
    return (key_heads, value_heads, -unit, write, decay)

def run_chain(state, queries, inputs, reverse):
    key_heads, value_heads, erase, write, decay = inputs

    def advance(carry, item):
        query, key_row, value_row, erase_row, write_row, decay_row = item
        removed = jnp.einsum('hij,hj->hi', carry, erase_row, precision=highest)
        carry = carry * decay_row[:, None, :] + removed[:, :, None] * write_row[:, None, :] + value_row[:, :, None] * key_row[:, None, :]
        return (carry, jnp.einsum('hij,hj->hi', carry, query, precision=highest))
    return lax.scan(advance, state, (queries, key_heads, value_heads, erase, write, decay), reverse=reverse)

def reference(latent, context, condition, context_condition, shift_weight, scale_weight, gate_weight, norm_gain, decay_down, decay_up, rate_down, rate_up, head_bias, query_weight, key_weight, value_weight, branch_weight, group_gain, out_weight):
    conditions = jax.nn.silu(jnp.stack([condition, context_condition])).astype(jnp.bfloat16)
    shift = jnp.dot(conditions, shift_weight, preferred_element_type=jnp.float32)
    scale = jnp.dot(conditions, scale_weight, preferred_element_type=jnp.float32)
    gate = jnp.dot(conditions[:1], gate_weight, preferred_element_type=jnp.float32)[0]
    normed = modulated(latent, norm_gain, scale[0], shift[0])
    normed_context = modulated(context, norm_gain, scale[1], shift[1])
    queries = jnp.dot(normed, query_weight, preferred_element_type=jnp.float32).astype(jnp.bfloat16)
    branch = jnp.dot(normed, branch_weight, preferred_element_type=jnp.float32).astype(jnp.bfloat16)
    latent_in = chain_inputs(*features(normed, key_weight, value_weight, decay_down, decay_up, rate_down, rate_up), head_bias)
    context_in = chain_inputs(*features(normed_context, key_weight, value_weight, decay_down, decay_up, rate_down, rate_up), head_bias)
    query_heads = queries.astype(jnp.float32).reshape(TOKENS, -1, HEAD_DIM)
    zero_state = jnp.zeros((D // HEAD_DIM, HEAD_DIM, HEAD_DIM), jnp.float32)
    reads = jnp.zeros((TOKENS, D // HEAD_DIM, HEAD_DIM), jnp.float32)
    for reverse in (False, True):
        carried, _ = run_chain(zero_state, context_in[0], context_in, reverse)
        _, latent_read = run_chain(carried, query_heads, latent_in, reverse)
        reads = reads + latent_read
    center = lax.optimization_barrier(jnp.mean(reads, axis=-1, keepdims=True))
    variance = lax.optimization_barrier(jnp.mean(jnp.square(reads - center), axis=-1, keepdims=True))
    normal_heads = ((reads - center) * lax.rsqrt(variance + GROUP_EPS)).reshape(TOKENS, D)
    mixed = (normal_heads * group_gain * jax.nn.silu(branch.astype(jnp.float32))).astype(jnp.bfloat16)
    width = D // N_TP
    summed = jnp.zeros((TOKENS, D), jnp.float32)
    for group in range(N_TP):
        partial_sum = jnp.dot(mixed[:, group * width:(group + 1) * width], out_weight[group * width:(group + 1) * width], preferred_element_type=jnp.float32)
        summed = summed + lax.optimization_barrier(partial_sum.astype(jnp.bfloat16)).astype(jnp.float32)
    mixer = summed.astype(jnp.bfloat16).astype(jnp.float32)
    normed_out = mixer * lax.rsqrt(lax.optimization_barrier(jnp.mean(mixer * mixer, axis=-1, keepdims=True)) + NORM_EPS)
    return (latent.astype(jnp.float32) + gate * normed_out).astype(jnp.bfloat16)
```

```python
import functools
import math

import jax
import jax.numpy as jnp
from jax import lax
from jax.experimental import pallas as pl
from jax.experimental.pallas import tpu as pltpu
from jax.sharding import PartitionSpec as P

HEAD_DIM = 64
NORM_EPS = 1e-06
GROUP_EPS = 0.00064
DECAY_TOP = math.exp(-0.5)
MESH = pl.DeviceIdType.MESH
bf16 = jnp.bfloat16
f32 = jnp.float32
LEN = 128
N_SP = 16
N_TP = 8
HALF = 64


def mm(a, b):
    return jnp.dot(a, b, preferred_element_type=f32)


def mm_nt(a, b):
    return lax.dot_general(a, b, (((1,), (1,)), ((), ())), preferred_element_type=f32)


def split(a):
    high = a.astype(bf16)
    return high, (a - high.astype(f32)).astype(bf16)


def rows_cols():
    row = lax.broadcasted_iota(jnp.int32, (LEN, LEN), 0)
    col = lax.broadcasted_iota(jnp.int32, (LEN, LEN), 1)
    return row, col


def cumulative(log_decay, row, col):
    lower = jnp.where(row >= col, 1.0, 0.0).astype(bf16)
    high, low = split(log_decay)
    return mm(lower, high) + mm(lower, low)


def solve(couplings, sides, cross):
    row, col = rows_cols()
    eye = jnp.where(row == col, 1.0, 0.0)
    inverse = [eye + jnp.where(cross == 1, a, 0.0) for a in couplings]
    size = 2
    while size < LEN // 2:
        level = (cross >= size) & (cross < 2 * size)
        low = [d.astype(bf16) for d in inverse]
        part = [mm(jnp.where(level, a, 0.0).astype(bf16), d) for a, d in zip(couplings, low)]
        inverse = [d + mm(e, p.astype(bf16)) for d, e, p in zip(inverse, low, part)]
        size *= 2
    level = (cross >= size) & (cross < 2 * size)
    low = [d.astype(bf16) for d in inverse]
    first = [mm(d, s.astype(bf16)) for d, s in zip(low, sides)]
    part = [
        mm(jnp.where(level, a, 0.0).astype(bf16), y.astype(bf16)) for a, y in zip(couplings, first)
    ]
    return [y + mm(d, p.astype(bf16)) for y, d, p in zip(first, low, part)]


def head_mask(head):
    lane = lax.broadcasted_iota(jnp.int32, (1, LEN), 1)
    return (lane >= HALF) if head else (lane < HALF)


def pair_unit(keys):
    own = head_mask(0)
    square = keys * keys
    sums = [
        jnp.sum(jnp.where(mask, square, 0.0), axis=-1, keepdims=True)
        for mask in (own, head_mask(1))
    ]
    return keys * lax.rsqrt(jnp.where(own, sums[0], sums[1]) + 1.0)


def state_map(transposed, solved, crossed, total, head):
    lo = head * HALF
    out = mm(
        transposed[lo : lo + HALF], jnp.concatenate([solved, crossed], axis=0)
    )
    row = lax.broadcasted_iota(jnp.int32, (HALF, LEN), 0)
    lane = lax.broadcasted_iota(jnp.int32, (HALF, LEN), 1)
    out = out + jnp.where(lane == row + lo, jnp.exp(total), 0.0)
    return pltpu.roll(out, HALF, 1) if head else out


def pair_terms(queries, keys, values, log_decay, rate):
    row, col = rows_cols()
    cross = row ^ col
    cum = cumulative(log_decay, row, col)
    total = cum[LEN - 1 : LEN]
    half = 0.5 * total
    scale = jnp.exp(half)
    unit = pair_unit(keys)
    erase = -unit
    write = unit * rate
    before = jnp.exp(cum - log_decay - half)
    after = jnp.exp(half - cum)
    step = jnp.exp(log_decay)
    crossed_values = pltpu.roll(values, HALF, 1)
    own = [head_mask(0), head_mask(1)]
    units = []
    for direction in (0, 1):
        left, right = (before, after) if direction == 0 else (after, before)
        er, qr = erase * left, queries * (left * step)
        wr, kr = write * right, keys * right
        right_both = jnp.concatenate([wr, kr], axis=0).astype(bf16)
        transposed = jnp.concatenate(
            [jnp.transpose(wr * scale), jnp.transpose(kr * scale)], axis=1
        ).astype(bf16)
        for head in (0, 1):
            left_both = jnp.concatenate(
                [jnp.where(own[head], er, 0.0), jnp.where(own[head], qr, 0.0)], axis=0
            ).astype(bf16)
            grams = mm_nt(left_both, right_both)
            strict = (row > col) if direction == 0 else (row < col)
            reach = (row >= col) if direction == 0 else (row <= col)
            coupling = jnp.where(strict, grams[:LEN, :LEN], 0.0)
            feeding = jnp.where(strict, grams[:LEN, LEN:], 0.0).astype(bf16)
            attend = jnp.where(
                jnp.concatenate([reach, reach], axis=1), grams[LEN:], 0.0
            ).astype(bf16)
            fed = mm(feeding, crossed_values.astype(bf16))
            side = jnp.where(own[head], er, fed)
            units.append((direction, head, coupling, side, attend, qr, transposed))
    answers = solve([u[2] for u in units], [u[3] for u in units], cross)
    maps = [[None, None], [None, None]]
    reads = [[None, None], [None, None]]
    for unit_terms, answer in zip(units, answers):
        direction, head, _, _, attend, qr, transposed = unit_terms
        mine = own[head]
        solved = jnp.where(mine, answer * scale, answer).astype(bf16)
        crossed = jnp.where(mine, 0.0, crossed_values).astype(bf16)
        maps[direction][head] = state_map(transposed, solved, crossed, total, head)
        reads[direction][head] = mm(
            attend, jnp.concatenate([solved, crossed], axis=0)
        ) + jnp.where(mine, qr * scale, 0.0)
    ahead = [jnp.where(own[0], r[0], r[1]) for r in reads]
    local = jnp.where(own[0], reads[0][1], reads[0][0]) + jnp.where(
        own[0], reads[1][1], reads[1][0]
    )
    return jnp.concatenate(ahead, axis=1), pltpu.roll(local, HALF, 1), maps


def context_terms(pairs, lows, bias, backward):
    row, col = rows_cols()
    cross = row ^ col
    own = head_mask(0)
    order = (row - col) * (1 - 2 * backward)
    strict = order > 0
    units = []
    for pair, low in zip(pairs, lows):
        gates = jax.nn.sigmoid(bias + low)
        log_decay = jnp.where(own, -DECAY_TOP * gates, 0.0)
        rate = pltpu.roll(gates, HALF, 1)
        keys = jnp.where(own, pair, 0.0)
        cum = cumulative(log_decay, row, col)
        total = cum[LEN - 1 : LEN]
        half = 0.5 * total
        scale = jnp.exp(half)
        unit = keys * lax.rsqrt(jnp.sum(keys * keys, axis=-1, keepdims=True) + 1.0)
        one, two = cum - log_decay - half, half - cum
        left = jnp.exp(jnp.where(backward == 0, one, two))
        right = jnp.exp(jnp.where(backward == 0, two, one))
        er, wr, kr = -unit * left, unit * rate * right, keys * right
        grams = mm_nt(er.astype(bf16), jnp.concatenate([wr, kr], axis=0).astype(bf16))
        coupling = jnp.where(strict, grams[:, :LEN], 0.0)
        feeding = jnp.where(strict, grams[:, LEN:], 0.0).astype(bf16)
        crossed = jnp.where(own, 0.0, pair).astype(bf16)
        side = jnp.where(own, er, mm(feeding, crossed))
        transposed = jnp.concatenate(
            [jnp.transpose(wr * scale), jnp.transpose(kr * scale)], axis=1
        ).astype(bf16)
        units.append((coupling, side, transposed, crossed, scale, total))
    answers = solve([u[0] for u in units], [u[1] for u in units], cross)
    maps = []
    for (_, _, transposed, crossed, scale, total), answer in zip(units, answers):
        solved = jnp.where(own, answer * scale, answer).astype(bf16)
        maps.append(state_map(transposed, solved, crossed, total, 0))
    return maps


def advance(state, step_map):
    high, low = split(state)
    transfer = step_map[:, :HALF]
    return mm(transfer, high) + mm(transfer, low) + step_map.astype(f32)


def remote(src, dst, send, recv, sp, tp):
    return pltpu.make_async_remote_copy(
        src_ref=src,
        dst_ref=dst,
        send_sem=send,
        recv_sem=recv,
        device_id=(sp, tp),
        device_id_type=MESH,
    )


def kernel(
    latent,
    context,
    condition,
    context_condition,
    shift_weight,
    scale_weight,
    gate_weight,
    norm_gain,
    decay_down,
    decay_up,
    rate_down,
    rate_up,
    head_bias,
    query_weight,
    key_weight,
    value_weight,
    branch_weight,
    group_gain,
    out_weight,
    out,
    rows,
    own_rows,
    ctx_rows,
    cond,
    mod_w,
    gain,
    down,
    up,
    bias,
    wq,
    wk,
    wv,
    wb,
    ggain,
    wo,
    part,
    ybuf,
    zpart,
    zbuf,
    mods,
    normed,
    low,
    kbuf,
    vbuf,
    dbuf,
    rbuf,
    qbuf,
    bbuf,
    ctx_out,
    ctx_in,
    head_rows,
    map_out,
    map_in,
    ctx_maps,
    ahead,
    local,
    state_out,
    states,
    mixed,
    partial,
    paired,
    summed,
    arrived,
    load,
    y_s,
    y_r,
    z_s,
    z_r,
    t_s,
    t_r,
    l_s,
    l_r,
    f_s,
    c_s,
    c_r,
    m_s,
    m_r,
    s_s,
    s_r,
    o_s,
    o_r,
    g_s,
    g_r,
):
    sp = lax.axis_index("sp")
    tp = lax.axis_index("tp")
    zz, yy = sp // 4, sp % 4
    xx, core = tp // 2, tp % 2
    sibling = 2 * xx + (1 - core)
    width = wq.shape[1]
    model = normed.shape[1]
    blocks = model // width
    own_n = own_rows.shape[0]
    ctx_n = ctx_rows.shape[0]

    barrier = pltpu.get_barrier_semaphore()

    def greet_sp(j, carry):
        pl.semaphore_signal(
            barrier, inc=1, device_id=((sp + j) % N_SP, tp), device_id_type=MESH
        )
        return carry

    def greet_tp(j, carry):
        pl.semaphore_signal(
            barrier, inc=1, device_id=(sp, (tp + j) % N_TP), device_id_type=MESH
        )
        return carry

    lax.fori_loop(1, N_SP, greet_sp, 0)
    lax.fori_loop(1, N_TP, greet_tp, 0)

    def fetch(at, src, dst):
        return pltpu.make_async_copy(src, dst, load.at[at])

    copies = [
        fetch(0, condition, cond.at[0:1]),
        fetch(1, context_condition, cond.at[1:2]),
        fetch(2, shift_weight, mod_w.at[0]),
        fetch(3, scale_weight, mod_w.at[1]),
        fetch(4, gate_weight, mod_w.at[2]),
        fetch(5, latent, own_rows),
        fetch(6, context, ctx_rows),
        fetch(7, norm_gain, gain),
        fetch(8, decay_down, down.at[:, 0:LEN]),
        fetch(9, rate_down, down.at[:, LEN : 2 * LEN]),
        fetch(10, decay_up, up.at[0]),
        fetch(11, rate_up, up.at[1]),
        fetch(12, head_bias, bias),
        fetch(13, key_weight, wk),
        fetch(14, value_weight, wv),
        fetch(15, query_weight, wq),
        fetch(16, branch_weight, wb),
        fetch(17, group_gain, ggain),
        fetch(18, out_weight, wo),
    ]
    for copy in copies:
        copy.start()

    for at in (0, 1, 2, 3, 4):
        copies[at].wait()
    rows_c = cond[...]
    conditions = (rows_c * jax.nn.sigmoid(rows_c)).astype(bf16)
    conditions = jnp.concatenate([conditions, jnp.zeros((14, rows_c.shape[1]), bf16)], axis=0)
    shares = [mm(conditions, mod_w[at]) for at in range(3)]
    part[...] = jnp.concatenate(
        [shares[0][0:2], shares[1][0:2], shares[2][0:1], jnp.zeros((3, width), f32)], axis=0
    )
    ybuf[yy] = part[...]
    pl.semaphore_wait(barrier, N_SP - 1 + N_TP - 1)

    sends = []

    def start(copy):
        copy.start()
        sends.append(copy)

    for j in (1, 2, 3):
        to = zz * 4 + (yy + j) % 4
        start(remote(part, ybuf.at[yy], y_s.at[j], y_r.at[yy], to, tp))
    copies[5].wait()
    for j in (2, 1, 3):
        to = 2 * ((xx + j) % 4) + core
        start(remote(own_rows, rows.at[tp], l_s.at[j], l_r.at[tp], sp, to))
    start(remote(own_rows, rows.at[tp], l_s.at[0], l_r.at[tp], sp, sibling))
    rows[tp] = own_rows[...]

    for j in (1, 2, 3):
        frm = (yy + j) % 4
        remote(part, ybuf.at[frm], y_s.at[j], y_r.at[frm], sp, tp).wait_recv()
    zpart[...] = ybuf[0] + ybuf[1] + ybuf[2] + ybuf[3]
    zbuf[zz] = zpart[...]
    for j in (1, 2, 3):
        to = ((zz + j) % 4) * 4 + yy
        start(remote(zpart, zbuf.at[zz], z_s.at[j], z_r.at[zz], to, tp))

    copies[6].wait()
    ctx = ctx_rows[...].astype(f32)
    ctx_scale = lax.rsqrt(jnp.mean(ctx * ctx, axis=-1, keepdims=True) + NORM_EPS)

    for j in (1, 2, 3):
        frm = (zz + j) % 4
        remote(zpart, zbuf.at[frm], z_s.at[j], z_r.at[frm], sp, tp).wait_recv()
    part2 = zbuf[0] + zbuf[1] + zbuf[2] + zbuf[3]
    mods[tp] = part2
    for j in range(1, N_TP):
        to = (tp + j) % N_TP
        start(remote(mods.at[tp], mods.at[tp], t_s.at[j], t_r.at[tp], sp, to))

    for j in (1, 3, 2):
        frm = 2 * ((xx + j) % 4) + core
        remote(own_rows, rows.at[frm], l_s.at[j], l_r.at[frm], sp, tp).wait_recv()
        start(remote(rows.at[frm], rows.at[frm], f_s.at[j], l_r.at[frm], sp, sibling))
    for j in (0, 1, 3, 2):
        frm = 2 * ((xx + j) % 4) + (1 - core)
        remote(own_rows, rows.at[frm], l_s.at[j], l_r.at[frm], sp, tp).wait_recv()
    inverses = []
    for i in range(N_TP):
        values = rows[i].astype(f32)
        inverses.append(lax.rsqrt(jnp.mean(values * values, axis=-1, keepdims=True) + NORM_EPS))

    copies[7].wait()
    for j in range(1, N_TP):
        frm = (tp + j) % N_TP
        remote(part, mods.at[frm], t_s.at[j], t_r.at[frm], sp, tp).wait_recv()

    for j in range(blocks):
        cols = slice(j * width, (j + 1) * width)
        vectors = mods[j]
        factor = gain[0:1, cols] * (1.0 + vectors[2:3])
        shift = vectors[0:1]
        for i in range(N_TP):
            normed[i * own_n : (i + 1) * own_n, cols] = (
                rows[i, :, cols].astype(f32) * inverses[i] * factor + shift
            ).astype(bf16)
        factor = gain[0:1, cols] * (1.0 + vectors[3:4])
        shift = vectors[1:2]
        normed[LEN : LEN + ctx_n, cols] = (
            ctx_rows[:, cols].astype(f32) * ctx_scale * factor + shift
        ).astype(bf16)

    for at in (8, 9, 10, 11, 12):
        copies[at].wait()
    lows = mm(normed[...], down[...])
    low[:, :LEN] = jnp.tanh(lows[:, :LEN]).astype(bf16)
    low[:, LEN:] = lows[:, LEN:].astype(bf16)
    dbuf[...] = mm(low[:, :LEN], up[0]).astype(bf16)
    rbuf[...] = mm(low[:, LEN:], up[1]).astype(bf16)

    def project(weight, to, count):
        def body(i, carry):
            at = pl.ds(pl.multiple_of(i * 256, 256), 256)
            to[:, at] = mm(normed[0:count], weight[:, at]).astype(bf16)
            return carry

        lax.fori_loop(0, width // 256, body, 0)

    copies[13].wait()
    project(wk, kbuf, LEN + ctx_n)
    copies[14].wait()
    project(wv, vbuf, LEN + ctx_n)

    lane = lax.broadcasted_iota(jnp.int32, (1, LEN), 1)
    left = lane < HALF
    for p in range(width // LEN):
        cols = slice(p * LEN, (p + 1) * LEN)
        for at, (first, second) in enumerate(((kbuf, vbuf), (dbuf, rbuf))):
            a = first[LEN : LEN + ctx_n, cols].astype(f32)
            b = second[LEN : LEN + ctx_n, cols].astype(f32)
            lanes = slice(at * LEN, (at + 1) * LEN)
            ctx_out[2 * p, :, lanes] = jnp.where(left, a, pltpu.roll(b, HALF, 1)).astype(bf16)
            ctx_out[2 * p + 1, :, lanes] = jnp.where(left, pltpu.roll(a, HALF, 1), b).astype(bf16)
        a = bias[0:1, cols]
        b = bias[1:2, cols]
        head_rows[2 * p : 2 * p + 1] = jnp.where(left, a, pltpu.roll(b, HALF, 1))
        head_rows[2 * p + 1 : 2 * p + 2] = jnp.where(left, pltpu.roll(a, HALF, 1), b)
    my_head = sp % 8
    backward = sp // 8
    ctx_in[sp] = ctx_out[my_head]

    def send_ctx(j, carry):
        to = (sp + j) % N_SP
        remote(ctx_out.at[to % 8], ctx_in.at[sp], c_s.at[j], c_r.at[sp], to, tp).start()
        return carry

    lax.fori_loop(1, N_SP, send_ctx, 0)

    copies[15].wait()
    project(wq, qbuf, LEN)
    copies[16].wait()
    project(wb, bbuf, LEN)

    def map_copy(to, carry=None):
        return remote(map_out.at[to], map_in.at[sp], m_s.at[to], m_r.at[sp], to, tp)

    def chunk(p, carry):
        at = pl.ds(pl.multiple_of(p * LEN, LEN), LEN)
        gates = jax.nn.sigmoid(bias[0:1, at] + dbuf[0:LEN, at].astype(f32))
        rate = jax.nn.sigmoid(bias[1:2, at] + rbuf[0:LEN, at].astype(f32))
        coming, here, maps = pair_terms(
            qbuf[:, at].astype(f32),
            kbuf[0:LEN, at].astype(f32),
            vbuf[0:LEN, at].astype(f32),
            -DECAY_TOP * gates,
            rate,
        )
        for direction in (0, 1):
            for head in (0, 1):
                map_out[direction * 8 + 2 * p + head] = maps[direction][head].astype(bf16)
        for direction in (0, 1):
            for head in (0, 1):
                to = direction * 8 + 2 * p + head

                @pl.when(to != sp)
                def _():
                    map_copy(to).start()

        ahead[p] = coming.astype(bf16)
        local[p] = here
        return carry

    lax.fori_loop(0, width // LEN, chunk, 0)
    map_in[sp] = map_out[sp]

    for j in range(1, N_SP):
        frm = (sp + j) % N_SP
        remote(ctx_out.at[0], ctx_in.at[frm], c_s.at[j], c_r.at[frm], sp, tp).wait_recv()
    my_bias = head_rows[pl.ds(my_head, 1)]
    per = LEN // ctx_n
    pairs, lows_in = [], []
    for c in range(N_SP // per):
        pairs.append(ctx_in[c * per : (c + 1) * per, :, 0:LEN].astype(f32).reshape(LEN, LEN))
        lows_in.append(ctx_in[c * per : (c + 1) * per, :, LEN:].astype(f32).reshape(LEN, LEN))
    for c, found in enumerate(context_terms(pairs, lows_in, my_bias, backward)):
        ctx_maps[c] = found
    count = N_SP // per
    forward = backward == 0
    state = ctx_maps[jnp.where(forward, 0, count - 1)]
    for c in range(1, count):
        state = advance(state, ctx_maps[jnp.where(forward, c, count - 1 - c)].astype(bf16))

    odd = my_head % 2
    keep = (lane >= HALF) == (odd == 1)

    def walk(i, state):
        at = jnp.where(forward, i, N_SP - 1 - i)
        shown = jnp.where(odd == 1, state, pltpu.roll(state, HALF, 1))
        state_out[at] = jnp.where(keep, shown, 0.0).astype(bf16)

        @pl.when(at != sp)
        def _():
            remote(state_out.at[at], states.at[sp], s_s.at[at], s_r.at[sp], at, tp).start()
            remote(map_out.at[0], map_in.at[at], m_s.at[at], m_r.at[at], sp, tp).wait_recv()

        return advance(state, map_in[at])

    lax.fori_loop(0, N_SP, walk, state)
    states[sp] = state_out[sp]
    for j in range(1, N_SP):
        frm = (sp + j) % N_SP
        remote(state_out.at[0], states.at[frm], s_s.at[0], s_r.at[frm], sp, tp).wait_recv()

    copies[17].wait()
    other = lane >= HALF
    for p in range(width // LEN):
        cols = slice(p * LEN, (p + 1) * LEN)
        both = jnp.concatenate(
            [
                states[2 * p : 2 * p + 2].reshape(LEN, LEN),
                states[8 + 2 * p : 8 + 2 * p + 2].reshape(LEN, LEN),
            ],
            axis=0,
        )
        reads = mm(ahead[p], both) + local[p]

        def head_mean(x):
            sums = [
                jnp.sum(jnp.where(mask, x, 0.0), axis=-1, keepdims=True) for mask in (left, other)
            ]
            return jnp.where(left, sums[0], sums[1]) * (1.0 / HALF)

        centred = reads - head_mean(reads)
        normal = centred * lax.rsqrt(head_mean(centred * centred) + GROUP_EPS)
        gate = bbuf[:, cols].astype(f32)
        mixed[:, cols] = (
            normal * ggain[0:1, cols] * (gate * jax.nn.sigmoid(gate))
        ).astype(bf16)

    copies[18].wait()
    n_chunk = arrived.shape[0]
    piece = model // n_chunk
    for c in range(n_chunk):
        cols = slice(c * piece, (c + 1) * piece)
        product = mm(mixed[...], wo[:, cols]).astype(bf16)
        for x in range(4):
            for k in range(2):
                lo = (2 * x + k) * own_n
                partial[c, k, x] = product[lo : lo + own_n]
        start(
            remote(
                partial.at[c, 1 - core], paired.at[c], o_s.at[c], o_r.at[c], sp, sibling
            )
        )
    for c in range(n_chunk):
        remote(partial.at[c, 0], paired.at[c], o_s.at[c], o_r.at[c], sp, tp).wait_recv()
        summed[c] = (partial[c, core].astype(f32) + paired[c].astype(f32)).astype(bf16)
        for j in (2, 1, 3):
            x = (xx + j) % 4
            start(
                remote(
                    summed.at[c, x], arrived.at[c, xx], g_s.at[c, j], g_r.at[c, xx], sp, 2 * x + core
                )
            )
        arrived[c, xx] = summed[c, xx]
    pieces = []
    for c in range(n_chunk):
        for j in (1, 3, 2):
            x = (xx + j) % 4
            remote(
                summed.at[c, 0], arrived.at[c, x], g_s.at[c, j], g_r.at[c, x], sp, tp
            ).wait_recv()
        total = arrived[c, 0].astype(f32)
        for x in range(1, 4):
            total = total + arrived[c, x].astype(f32)
        pieces.append(total.astype(bf16).astype(f32))
    square = sum(jnp.sum(p * p, axis=-1, keepdims=True) for p in pieces)
    inverse = lax.rsqrt(square * (1.0 / model) + NORM_EPS)
    for c in range(n_chunk):
        for s in range(piece // width):
            j = c * (piece // width) + s
            cols = slice(j * width, (j + 1) * width)
            value = pieces[c][:, s * width : (s + 1) * width]
            out[:, cols] = (
                own_rows[:, cols].astype(f32) + mods[j, 4:5] * (value * inverse)
            ).astype(bf16)

    for copy in sends:
        copy.wait_send()

    def drain_ctx(j, carry):
        remote(ctx_out.at[0], ctx_in.at[0], c_s.at[j], c_r.at[0], sp, tp).wait_send()
        to = (sp + j) % N_SP
        remote(map_out.at[0], map_in.at[0], m_s.at[to], m_r.at[0], sp, tp).wait_send()
        remote(state_out.at[0], states.at[0], s_s.at[to], s_r.at[0], sp, tp).wait_send()
        return carry

    lax.fori_loop(1, N_SP, drain_ctx, 0)


def on_device(
    latent,
    context,
    condition,
    context_condition,
    shift_weight,
    scale_weight,
    gate_weight,
    norm_gain,
    decay_down,
    decay_up,
    rate_down,
    rate_up,
    head_bias,
    query_weight,
    key_weight,
    value_weight,
    branch_weight,
    group_gain,
    out_weight,
):
    own_n, model = latent.shape
    ctx_n = context.shape[0]
    width = query_weight.shape[1]
    held = condition.shape[0]
    args = (
        latent,
        context,
        condition.reshape(1, -1),
        context_condition.reshape(1, -1),
        shift_weight,
        scale_weight,
        gate_weight,
        norm_gain.reshape(1, -1),
        decay_down,
        decay_up,
        rate_down,
        rate_up,
        head_bias,
        query_weight,
        key_weight,
        value_weight,
        branch_weight,
        group_gain.reshape(1, -1),
        out_weight,
    )
    n_chunk = 4
    piece = model // n_chunk
    V = pltpu.VMEM
    dma = pltpu.SemaphoreType.DMA
    scratch = [
        V((N_TP, own_n, model), bf16),
        V((own_n, model), bf16),
        V((ctx_n, model), bf16),
        V((2, held), f32),
        V((3, held, width), bf16),
        V((1, model), f32),
        V((model, 2 * LEN), bf16),
        V((2, LEN, width), bf16),
        V((2, width), f32),
        V((model, width), bf16),
        V((model, width), bf16),
        V((model, width), bf16),
        V((model, width), bf16),
        V((1, width), f32),
        V((width, model), bf16),
        V((8, width), f32),
        V((4, 8, width), f32),
        V((8, width), f32),
        V((4, 8, width), f32),
        V((N_TP, 8, width), f32),
        V((LEN + ctx_n, model), bf16),
        V((LEN + ctx_n, 2 * LEN), bf16),
        V((LEN + ctx_n, width), bf16),
        V((LEN + ctx_n, width), bf16),
        V((LEN + ctx_n, width), bf16),
        V((LEN + ctx_n, width), bf16),
        V((LEN, width), bf16),
        V((LEN, width), bf16),
        V((8, ctx_n, 2 * LEN), bf16),
        V((N_SP, ctx_n, 2 * LEN), bf16),
        V((8, LEN), f32),
        V((N_SP, HALF, LEN), bf16),
        V((N_SP, HALF, LEN), bf16),
        V((4, HALF, LEN), f32),
        V((width // LEN, LEN, 2 * LEN), bf16),
        V((width // LEN, LEN, LEN), f32),
        V((N_SP, HALF, LEN), bf16),
        V((N_SP, HALF, LEN), bf16),
        V((LEN, width), bf16),
        V((n_chunk, 2, 4, own_n, piece), bf16),
        V((n_chunk, 4, own_n, piece), bf16),
        V((n_chunk, 4, own_n, piece), bf16),
        V((n_chunk, 4, own_n, piece), bf16),
        dma((19,)),
        dma((4,)),
        dma((4,)),
        dma((4,)),
        dma((4,)),
        dma((N_TP,)),
        dma((N_TP,)),
        dma((4,)),
        dma((N_TP,)),
        dma((4,)),
        dma((N_SP,)),
        dma((N_SP,)),
        dma((N_SP,)),
        dma((N_SP,)),
        dma((N_SP,)),
        dma((N_SP,)),
        dma((n_chunk,)),
        dma((n_chunk,)),
        dma((n_chunk, 4)),
        dma((n_chunk, 4)),
    ]
    return pl.pallas_call(
        kernel,
        out_shape=jax.ShapeDtypeStruct((own_n, model), bf16),
        in_specs=[pl.BlockSpec(memory_space=pl.ANY)] * len(args),
        out_specs=pl.BlockSpec(memory_space=pltpu.VMEM),
        scratch_shapes=scratch,
        compiler_params=pltpu.CompilerParams(
            collective_id=0, has_side_effects=True, vmem_limit_bytes=60 * 1024 * 1024
        ),
    )(*args)


def solution(mesh):
    placed = (
        P(("sp", "tp"), None),
        P("sp", None),
        P("sp"),
        P("sp"),
        P("sp", "tp"),
        P("sp", "tp"),
        P("sp", "tp"),
        P(),
        P(),
        P(None, "tp"),
        P(),
        P(None, "tp"),
        P(None, "tp"),
        P(None, "tp"),
        P(None, "tp"),
        P(None, "tp"),
        P(None, "tp"),
        P("tp"),
        P("tp", None),
    )
    return jax.shard_map(
        on_device, mesh=mesh, in_specs=placed, out_specs=P(("sp", "tp"), None), check_vma=False
    )
```

```python
import contextlib
import math

import jax
import jax.numpy as jnp
from jax import lax
from jax.experimental import pallas as pl
from jax.experimental.pallas import tpu as pltpu
from jax.sharding import PartitionSpec as P

HEAD_DIM = 64
NORM_EPS = 1e-06
GROUP_EPS = 0.00064
DECAY_TOP = math.exp(-0.5)
MESH = pl.DeviceIdType.MESH
bf16 = jnp.bfloat16
f32 = jnp.float32
LEN = 128
group = 2
lag = 5
N_SP = 16
N_TP = 8
HALF = 64


def mm(a, b):
    return jnp.dot(a, b, preferred_element_type=f32)


def mm_nt(a, b):
    return lax.dot_general(a, b, (((1,), (1,)), ((), ())), preferred_element_type=f32)


def split(a):
    high = a.astype(bf16)
    return high, (a - high.astype(f32)).astype(bf16)


def rows_cols():
    row = lax.broadcasted_iota(jnp.int32, (LEN, LEN), 0)
    col = lax.broadcasted_iota(jnp.int32, (LEN, LEN), 1)
    return row, col


def cumulative(log_decay, row, col):
    lower = jnp.where(row >= col, 1.0, 0.0).astype(bf16)
    high, low = split(log_decay)
    return mm(lower, high) + mm(lower, low)


def solve(couplings, sides, cross):
    row, col = rows_cols()
    eye = jnp.where(row == col, 1.0, 0.0)
    inverse = [eye + jnp.where(cross == 1, a, 0.0) for a in couplings]
    size = 2
    while size < LEN // 2:
        level = (cross >= size) & (cross < 2 * size)
        low = [d.astype(bf16) for d in inverse]
        part = [mm(jnp.where(level, a, 0.0).astype(bf16), d) for a, d in zip(couplings, low)]
        inverse = [d + mm(e, p.astype(bf16)) for d, e, p in zip(inverse, low, part)]
        size *= 2
    level = (cross >= size) & (cross < 2 * size)
    low = [d.astype(bf16) for d in inverse]
    first = [mm(d, s.astype(bf16)) for d, s in zip(low, sides)]
    part = [
        mm(jnp.where(level, a, 0.0).astype(bf16), y.astype(bf16)) for a, y in zip(couplings, first)
    ]
    return [y + mm(d, p.astype(bf16)) for y, d, p in zip(first, low, part)]


def head_mask(head):
    lane = lax.broadcasted_iota(jnp.int32, (1, LEN), 1)
    return (lane >= HALF) if head else (lane < HALF)


def pair_unit(keys):
    own = head_mask(0)
    square = keys * keys
    sums = [
        jnp.sum(jnp.where(mask, square, 0.0), axis=-1, keepdims=True)
        for mask in (own, head_mask(1))
    ]
    return keys * lax.rsqrt(jnp.where(own, sums[0], sums[1]) + 1.0)


def state_map(transposed, solved, crossed, total, head):
    lo = head * HALF
    out = mm(
        transposed[lo : lo + HALF], jnp.concatenate([solved, crossed], axis=0)
    )
    row = lax.broadcasted_iota(jnp.int32, (HALF, LEN), 0)
    lane = lax.broadcasted_iota(jnp.int32, (HALF, LEN), 1)
    out = out + jnp.where(lane == row + lo, jnp.exp(total), 0.0)
    return pltpu.roll(out, HALF, 1) if head else out


def pair_setup(keys, values, log_decay, rate, row, col):
    cum = cumulative(log_decay, row, col)
    total = cum[LEN - 1 : LEN]
    half = 0.5 * total
    scale = jnp.exp(half)
    unit = pair_unit(keys)
    erase = -unit
    write = unit * rate
    before = jnp.exp(cum - log_decay - half)
    after = jnp.exp(half - cum)
    step = jnp.exp(log_decay)
    crossed_values = pltpu.roll(values, HALF, 1)
    fed_by = crossed_values.astype(bf16)
    own = [head_mask(0), head_mask(1)]
    units, rights, factors = [], [], []
    for direction in (0, 1):
        left, right = (before, after) if direction == 0 else (after, before)
        er = erase * left
        wr, kr = write * right, keys * right
        right_both = jnp.concatenate([wr, kr], axis=0).astype(bf16)
        rights.append(right_both)
        factors.append(left * step)
        transposed = jnp.concatenate(
            [jnp.transpose(wr * scale), jnp.transpose(kr * scale)], axis=1
        ).astype(bf16)
        left_both = jnp.concatenate([jnp.where(mask, er, 0.0) for mask in own], axis=0)
        grams = mm_nt(left_both.astype(bf16), right_both)
        strict = (row > col) if direction == 0 else (row < col)
        for head in (0, 1):
            rows = slice(head * LEN, (head + 1) * LEN)
            coupling = jnp.where(strict, grams[rows, :LEN], 0.0)
            feeding = jnp.where(strict, grams[rows, LEN:], 0.0).astype(bf16)
            side = jnp.where(own[head], er, mm(feeding, fed_by))
            units.append((coupling, side, transposed, head))
    return units, rights, factors, crossed_values, scale, total


def pairs_terms(inputs):
    row, col = rows_cols()
    setups = [pair_setup(*given, row, col) for given in inputs]
    flat = [unit for setup in setups for unit in setup[0]]
    answers = solve([u[0] for u in flat], [u[1] for u in flat], row ^ col)
    results, at = [], 0
    for units, rights, factors, crossed_values, scale, total in setups:
        maps, solved = [], []
        for _, _, transposed, head in units:
            mine = head_mask(head)
            answer = answers[at]
            at += 1
            rows = jnp.where(mine, answer * scale, answer).astype(bf16)
            crossed = jnp.where(mine, 0.0, crossed_values).astype(bf16)
            maps.append(state_map(transposed, rows, crossed, total, head))
            solved.append(rows)
        results.append((maps, solved, rights, factors, scale))
    return results


def pair_reads(queries, values, solved, rights, factors, scale):
    row, col = rows_cols()
    own = [head_mask(0), head_mask(1)]
    crossed_values = pltpu.roll(values, HALF, 1)
    crossed = [jnp.where(mask, 0.0, crossed_values).astype(bf16) for mask in own]
    reads = []
    for direction in (0, 1):
        qr = queries * factors[direction]
        left_both = jnp.concatenate([jnp.where(mask, qr, 0.0) for mask in own], axis=0)
        grams = mm_nt(left_both.astype(bf16), rights[direction])
        reach = (row >= col) if direction == 0 else (row <= col)
        both = jnp.concatenate([reach, reach], axis=1)
        for head in (0, 1):
            attend = jnp.where(both, grams[head * LEN : (head + 1) * LEN], 0.0).astype(bf16)
            reads.append(
                mm(attend, jnp.concatenate([solved[2 * direction + head], crossed[head]], axis=0))
                + jnp.where(own[head], qr * scale, 0.0)
            )
    ahead = [jnp.where(own[0], reads[at], reads[at + 1]) for at in (0, 2)]
    local = jnp.where(own[0], reads[1], reads[0]) + jnp.where(own[0], reads[3], reads[2])
    return jnp.concatenate(ahead, axis=1), pltpu.roll(local, HALF, 1)


def context_terms(pairs, lows, bias, backward):
    row, col = rows_cols()
    cross = row ^ col
    own = head_mask(0)
    order = (row - col) * (1 - 2 * backward)
    strict = order > 0
    units = []
    for pair, low in zip(pairs, lows):
        gates = jax.nn.sigmoid(bias + low)
        log_decay = jnp.where(own, -DECAY_TOP * gates, 0.0)
        rate = pltpu.roll(gates, HALF, 1)
        keys = jnp.where(own, pair, 0.0)
        cum = cumulative(log_decay, row, col)
        total = cum[LEN - 1 : LEN]
        half = 0.5 * total
        scale = jnp.exp(half)
        unit = keys * lax.rsqrt(jnp.sum(keys * keys, axis=-1, keepdims=True) + 1.0)
        one, two = cum - log_decay - half, half - cum
        left = jnp.exp(jnp.where(backward == 0, one, two))
        right = jnp.exp(jnp.where(backward == 0, two, one))
        er, wr, kr = -unit * left, unit * rate * right, keys * right
        grams = mm_nt(er.astype(bf16), jnp.concatenate([wr, kr], axis=0).astype(bf16))
        coupling = jnp.where(strict, grams[:, :LEN], 0.0)
        feeding = jnp.where(strict, grams[:, LEN:], 0.0).astype(bf16)
        crossed = jnp.where(own, 0.0, pair).astype(bf16)
        side = jnp.where(own, er, mm(feeding, crossed))
        transposed = jnp.concatenate(
            [jnp.transpose(wr * scale), jnp.transpose(kr * scale)], axis=1
        ).astype(bf16)
        units.append((coupling, side, transposed, crossed, scale, total))
    answers = solve([u[0] for u in units], [u[1] for u in units], cross)
    maps = []
    for (_, _, transposed, crossed, scale, total), answer in zip(units, answers):
        solved = jnp.where(own, answer * scale, answer).astype(bf16)
        maps.append(state_map(transposed, solved, crossed, total, 0))
    return maps


def compose(earlier, later):
    high, low = split(earlier)
    transfer = later[:, :HALF].astype(bf16)
    lane = lax.broadcasted_iota(jnp.int32, (1, LEN), 1)
    return mm(transfer, high) + mm(transfer, low) + jnp.where(lane >= HALF, later, 0.0)


def remote(src, dst, send, recv, sp, tp):
    return pltpu.make_async_remote_copy(
        src_ref=src,
        dst_ref=dst,
        send_sem=send,
        recv_sem=recv,
        device_id=(sp, tp),
        device_id_type=MESH,
    )


def kernel(
    latent,
    context,
    condition,
    context_condition,
    shift_weight,
    scale_weight,
    gate_weight,
    norm_gain,
    decay_down,
    decay_up,
    rate_down,
    rate_up,
    head_bias,
    query_weight,
    key_weight,
    value_weight,
    branch_weight,
    group_gain,
    out_weight,
    out,
    rows,
    own_rows,
    ctx_rows,
    cond,
    mod_w,
    gain,
    down,
    up,
    bias,
    wq,
    wk,
    wv,
    wb,
    ggain,
    wo,
    part,
    ybuf,
    zpart,
    zbuf,
    mods,
    normed,
    low,
    kbuf,
    vbuf,
    dbuf,
    rbuf,
    qbuf,
    bbuf,
    ctx_out,
    ctx_in,
    head_rows,
    map_out,
    map_in,
    ctx_maps,
    solved_buf,
    right_buf,
    factor_buf,
    scale_buf,
    ahead,
    local,
    state_out,
    states,
    mixed,
    partial,
    paired,
    summed,
    arrived,
    load,
    y_s,
    y_r,
    z_s,
    z_r,
    t_s,
    t_r,
    l_s,
    l_r,
    f_s,
    c_s,
    c_r,
    m_s,
    m_r,
    s_s,
    s_r,
    o_s,
    o_r,
    g_s,
    g_r,
):
    sp = lax.axis_index("sp")
    tp = lax.axis_index("tp")
    zz, yy = sp // 4, sp % 4
    xx, core = tp // 2, tp % 2
    sibling = 2 * xx + (1 - core)
    width = wq.shape[1]
    model = normed.shape[1]
    blocks = model // width
    own_n = own_rows.shape[0]
    ctx_n = ctx_rows.shape[0]

    scopes = contextlib.ExitStack()

    def phase(name):
        scopes.close()
        scopes.enter_context(jax.named_scope(name))

    phase("greet")
    barrier = pltpu.get_barrier_semaphore()

    def greet_sp(j, carry):
        pl.semaphore_signal(
            barrier, inc=1, device_id=((sp + j) % N_SP, tp), device_id_type=MESH
        )
        return carry

    def greet_tp(j, carry):
        pl.semaphore_signal(
            barrier, inc=1, device_id=(sp, (tp + j) % N_TP), device_id_type=MESH
        )
        return carry

    lax.fori_loop(1, N_SP, greet_sp, 0)
    lax.fori_loop(1, N_TP, greet_tp, 0)

    def fetch(at, src, dst):
        return pltpu.make_async_copy(src, dst, load.at[at])

    copies = [
        fetch(0, condition, cond.at[0:1]),
        fetch(1, context_condition, cond.at[1:2]),
        fetch(2, shift_weight, mod_w.at[0]),
        fetch(3, scale_weight, mod_w.at[1]),
        fetch(4, gate_weight, mod_w.at[2]),
        fetch(5, latent, own_rows),
        fetch(6, context, ctx_rows),
        fetch(7, norm_gain, gain),
        fetch(8, decay_down, down.at[:, 0:LEN]),
        fetch(9, rate_down, down.at[:, LEN : 2 * LEN]),
        fetch(10, decay_up, up.at[0]),
        fetch(11, rate_up, up.at[1]),
        fetch(12, head_bias, bias),
        fetch(13, key_weight, wk),
        fetch(14, value_weight, wv),
        fetch(15, query_weight, wq),
        fetch(16, branch_weight, wb),
        fetch(17, group_gain, ggain),
        fetch(18, out_weight, wo),
    ]
    for copy in copies:
        copy.start()

    phase("wait_mod_w")
    for at in (0, 1, 2, 3, 4):
        copies[at].wait()
    phase("shares")
    rows_c = cond[...]
    conditions = (rows_c * jax.nn.sigmoid(rows_c)).astype(bf16)
    conditions = jnp.concatenate([conditions, jnp.zeros((14, rows_c.shape[1]), bf16)], axis=0)
    shares = [mm(conditions, mod_w[at]) for at in range(3)]
    part[...] = jnp.concatenate(
        [shares[0][0:2], shares[1][0:2], shares[2][0:1], jnp.zeros((3, width), f32)], axis=0
    )
    ybuf[yy] = part[...]
    phase("barrier")
    pl.semaphore_wait(barrier, N_SP - 1 + N_TP - 1)

    phase("send_y")
    sends = []

    def start(copy):
        copy.start()
        sends.append(copy)

    for j in (1, 2, 3):
        to = zz * 4 + (yy + j) % 4
        start(remote(part, ybuf.at[yy], y_s.at[j], y_r.at[yy], to, tp))
    copies[5].wait()
    for j in (2, 1, 3):
        to = 2 * ((xx + j) % 4) + core
        start(remote(own_rows, rows.at[tp], l_s.at[j], l_r.at[tp], sp, to))
    start(remote(own_rows, rows.at[tp], l_s.at[0], l_r.at[tp], sp, sibling))
    rows[tp] = own_rows[...]

    phase("wait_y")
    for j in (1, 2, 3):
        frm = (yy + j) % 4
        remote(part, ybuf.at[frm], y_s.at[j], y_r.at[frm], sp, tp).wait_recv()
    zpart[...] = ybuf[0] + ybuf[1] + ybuf[2] + ybuf[3]
    zbuf[zz] = zpart[...]
    for j in (1, 2, 3):
        to = ((zz + j) % 4) * 4 + yy
        start(remote(zpart, zbuf.at[zz], z_s.at[j], z_r.at[zz], to, tp))

    phase("ctx_stats")
    copies[6].wait()
    ctx = ctx_rows[...].astype(f32)
    ctx_scale = lax.rsqrt(jnp.mean(ctx * ctx, axis=-1, keepdims=True) + NORM_EPS)

    phase("wait_z")
    for j in (1, 2, 3):
        frm = (zz + j) % 4
        remote(zpart, zbuf.at[frm], z_s.at[j], z_r.at[frm], sp, tp).wait_recv()
    part2 = zbuf[0] + zbuf[1] + zbuf[2] + zbuf[3]
    mods[tp] = part2
    for j in range(1, N_TP):
        to = (tp + j) % N_TP
        start(remote(mods.at[tp], mods.at[tp], t_s.at[j], t_r.at[tp], sp, to))

    phase("latent_x")
    for j in (1, 3, 2):
        frm = 2 * ((xx + j) % 4) + core
        remote(own_rows, rows.at[frm], l_s.at[j], l_r.at[frm], sp, tp).wait_recv()
        start(remote(rows.at[frm], rows.at[frm], f_s.at[j], l_r.at[frm], sp, sibling))
    phase("latent_core")
    for j in (0, 1, 3, 2):
        frm = 2 * ((xx + j) % 4) + (1 - core)
        remote(own_rows, rows.at[frm], l_s.at[j], l_r.at[frm], sp, tp).wait_recv()
    phase("latent_stats")
    inverses = []
    for i in range(N_TP):
        values = rows[i].astype(f32)
        inverses.append(lax.rsqrt(jnp.mean(values * values, axis=-1, keepdims=True) + NORM_EPS))

    phase("wait_t")
    copies[7].wait()
    for j in range(1, N_TP):
        frm = (tp + j) % N_TP
        remote(part, mods.at[frm], t_s.at[j], t_r.at[frm], sp, tp).wait_recv()

    phase("normalize")
    for j in range(blocks):
        cols = slice(j * width, (j + 1) * width)
        vectors = mods[j]
        factor = gain[0:1, cols] * (1.0 + vectors[2:3])
        shift = vectors[0:1]
        for i in range(N_TP):
            normed[i * own_n : (i + 1) * own_n, cols] = (
                rows[i, :, cols].astype(f32) * inverses[i] * factor + shift
            ).astype(bf16)
        factor = gain[0:1, cols] * (1.0 + vectors[3:4])
        shift = vectors[1:2]
        normed[LEN : LEN + ctx_n, cols] = (
            ctx_rows[:, cols].astype(f32) * ctx_scale * factor + shift
        ).astype(bf16)

    phase("lows")
    for at in (8, 9, 10, 11, 12):
        copies[at].wait()
    lows = mm(normed[...], down[...])
    low[:, :LEN] = jnp.tanh(lows[:, :LEN]).astype(bf16)
    low[:, LEN:] = lows[:, LEN:].astype(bf16)
    dbuf[...] = mm(low[:, :LEN], up[0]).astype(bf16)
    rbuf[...] = mm(low[:, LEN:], up[1]).astype(bf16)

    def project(weight, to, count):
        def body(i, carry):
            at = pl.ds(pl.multiple_of(i * 256, 256), 256)
            to[:, at] = mm(normed[0:count], weight[:, at]).astype(bf16)
            return carry

        lax.fori_loop(0, width // 256, body, 0)

    phase("proj_kv")
    copies[13].wait()
    project(wk, kbuf, LEN + ctx_n)
    copies[14].wait()
    project(wv, vbuf, LEN + ctx_n)

    phase("ctx_pack")
    lane = lax.broadcasted_iota(jnp.int32, (1, LEN), 1)
    left = lane < HALF
    for p in range(width // LEN):
        cols = slice(p * LEN, (p + 1) * LEN)
        for at, (first, second) in enumerate(((kbuf, vbuf), (dbuf, rbuf))):
            a = first[LEN : LEN + ctx_n, cols].astype(f32)
            b = second[LEN : LEN + ctx_n, cols].astype(f32)
            lanes = slice(at * LEN, (at + 1) * LEN)
            ctx_out[2 * p, :, lanes] = jnp.where(left, a, pltpu.roll(b, HALF, 1)).astype(bf16)
            ctx_out[2 * p + 1, :, lanes] = jnp.where(left, pltpu.roll(a, HALF, 1), b).astype(bf16)
        a = bias[0:1, cols]
        b = bias[1:2, cols]
        head_rows[2 * p : 2 * p + 1] = jnp.where(left, a, pltpu.roll(b, HALF, 1))
        head_rows[2 * p + 1 : 2 * p + 2] = jnp.where(left, pltpu.roll(a, HALF, 1), b)
    my_head = sp % 8
    backward = sp // 8
    ctx_in[sp] = ctx_out[my_head]

    def send_ctx(j, carry):
        to = (sp + j) % N_SP
        remote(ctx_out.at[to % 8], ctx_in.at[sp], c_s.at[j], c_r.at[sp], to, tp).start()
        return carry

    lax.fori_loop(1, N_SP, send_ctx, 0)

    phase("chunks")
    def place(to):
        slot = jnp.where(to == sp, N_SP, sp)
        return slot, jnp.where(to == sp, sibling, tp)

    def chunk(g, carry):
        inputs, at = [], []
        for k in range(group):
            p = g * group + k
            cols = pl.ds(pl.multiple_of(p * LEN, LEN), LEN)
            gates = jax.nn.sigmoid(bias[0:1, cols] + dbuf[0:LEN, cols].astype(f32))
            rate = jax.nn.sigmoid(bias[1:2, cols] + rbuf[0:LEN, cols].astype(f32))
            inputs.append(
                (
                    kbuf[0:LEN, cols].astype(f32),
                    vbuf[0:LEN, cols].astype(f32),
                    -DECAY_TOP * gates,
                    rate,
                )
            )
            at.append(p)
        found = pairs_terms(inputs)
        for p, (maps, solved, rights, factors, scale) in zip(at, found):
            for direction in (0, 1):
                for head in (0, 1):
                    map_out[direction * 8 + 2 * p + head] = maps[2 * direction + head].astype(bf16)
        for p, (maps, solved, rights, factors, scale) in zip(at, found):
            for direction in (0, 1):
                for head in (0, 1):
                    to = direction * 8 + 2 * p + head
                    slot, over = place(to)
                    remote(
                        map_out.at[to], map_in.at[slot], m_s.at[to], m_r.at[slot], to, over
                    ).start()
                    solved_buf[p, 2 * direction + head] = solved[2 * direction + head]
                right_buf[p, direction] = rights[direction]
                factor_buf[p, direction] = factors[direction]
            scale_buf[p] = scale
        return carry

    lax.fori_loop(0, width // LEN // group, chunk, 0)
    map_in[sp] = map_out[sp]

    phase("wait_ctx")
    for j in range(1, N_SP):
        frm = (sp + j) % N_SP
        remote(ctx_out.at[0], ctx_in.at[frm], c_s.at[j], c_r.at[frm], sp, tp).wait_recv()
    phase("ctx_chunks")
    my_bias = head_rows[pl.ds(my_head, 1)]
    per = LEN // ctx_n
    pairs, lows_in = [], []
    for c in range(N_SP // per):
        pairs.append(ctx_in[c * per : (c + 1) * per, :, 0:LEN].astype(f32).reshape(LEN, LEN))
        lows_in.append(ctx_in[c * per : (c + 1) * per, :, LEN:].astype(f32).reshape(LEN, LEN))
    for c, found in enumerate(context_terms(pairs, lows_in, my_bias, backward)):
        ctx_maps[c] = found
    phase("wait_maps")
    for j in range(1, N_SP + 1):
        frm = (sp + j) % N_SP if j < N_SP else N_SP
        remote(map_out.at[0], map_in.at[frm], m_s.at[0], m_r.at[frm], sp, tp).wait_recv()
    phase("walk")
    count = N_SP // per
    forward = backward == 0
    order = [jnp.where(forward, i, N_SP - 1 - i) for i in range(N_SP)]
    steps = [map_in[order[i]].astype(f32) for i in range(N_SP - 1)]
    state = ctx_maps[jnp.where(forward, 0, count - 1)]
    for c in range(1, count):
        state = compose(state, ctx_maps[jnp.where(forward, c, count - 1 - c)])
    two = [compose(steps[2 * i], steps[2 * i + 1]) for i in range(7)]
    four = [compose(two[2 * i], two[2 * i + 1]) for i in range(3)]
    eight = compose(four[0], four[1])
    odd = my_head % 2
    left = lax.broadcasted_iota(jnp.int32, (1, LEN), 1) < HALF

    def show(i, state):
        to = order[i]
        state_out[to] = jnp.where(
            left, pltpu.roll(state[: HALF // 2], HALF, 1), state[HALF // 2 :]
        ).astype(bf16)

    def launch(i):
        to = order[i]
        slot, over = place(to)
        remote(state_out.at[to], states.at[slot], s_s.at[to], s_r.at[slot], to, over).start()

    held = {0: state}
    show(0, state)
    held[8] = compose(state, eight)
    held[4] = compose(state, four[0])
    show(8, held[8])
    show(4, held[4])
    for i in (0, 8, 4):
        launch(i)
    held[12] = compose(held[8], four[2])
    held[2] = compose(state, two[0])
    held[6] = compose(held[4], two[2])
    held[10] = compose(held[8], two[4])
    held[14] = compose(held[12], two[6])
    for i in (2, 6, 10, 12, 14):
        show(i, held[i])
    for i in (2, 6, 10, 12, 14):
        launch(i)
    for i in range(1, N_SP, 2):
        show(i, compose(held[i - 1], steps[i - 1]))
    for i in range(1, N_SP, 2):
        launch(i)
    states[sp] = state_out[sp]

    phase("proj_qb")
    copies[15].wait()
    project(wq, qbuf, LEN)
    copies[16].wait()
    project(wb, bbuf, LEN)

    phase("read_terms")

    def read_terms(p, carry):
        cols = pl.ds(pl.multiple_of(p * LEN, LEN), LEN)
        coming, here = pair_reads(
            qbuf[:, cols].astype(f32),
            vbuf[0:LEN, cols].astype(f32),
            [solved_buf[p, i] for i in range(4)],
            [right_buf[p, i] for i in range(2)],
            [factor_buf[p, i] for i in range(2)],
            scale_buf[p],
        )
        ahead[p] = coming.astype(bf16)
        local[p] = here
        return carry

    lax.fori_loop(0, width // LEN, read_terms, 0)

    phase("wait_states")
    for j in range(1, N_SP + 1):
        frm = (sp + j) % N_SP if j < N_SP else N_SP
        remote(state_out.at[0], states.at[frm], s_s.at[0], s_r.at[frm], sp, tp).wait_recv()

    phase("reads")
    copies[17].wait()
    other = lane >= HALF
    for p in range(width // LEN):
        cols = slice(p * LEN, (p + 1) * LEN)
        blocks_in = []
        for at in (2 * p, 8 + 2 * p):
            first, second = states[at].astype(f32), states[at + 1].astype(f32)
            blocks_in += [
                jnp.where(left, first, 0.0),
                jnp.where(left, pltpu.roll(first, HALF, 1), 0.0),
                jnp.where(left, 0.0, pltpu.roll(second, HALF, 1)),
                jnp.where(left, 0.0, second),
            ]
        both = jnp.concatenate(blocks_in, axis=0).astype(bf16)
        reads = mm(ahead[p], both) + local[p]

        def head_mean(x):
            sums = [
                jnp.sum(jnp.where(mask, x, 0.0), axis=-1, keepdims=True) for mask in (left, other)
            ]
            return jnp.where(left, sums[0], sums[1]) * (1.0 / HALF)

        centred = reads - head_mean(reads)
        normal = centred * lax.rsqrt(head_mean(centred * centred) + GROUP_EPS)
        gate = bbuf[:, cols].astype(f32)
        mixed[:, cols] = (
            normal * ggain[0:1, cols] * (gate * jax.nn.sigmoid(gate))
        ).astype(bf16)

    phase("out_proj")
    copies[18].wait()
    n_chunk = arrived.shape[0]
    piece = model // n_chunk

    def pass_on(c):
        remote(partial.at[c, 0], paired.at[c], o_s.at[c], o_r.at[c], sp, tp).wait_recv()
        summed[c] = (partial[c, core].astype(f32) + paired[c].astype(f32)).astype(bf16)
        for j in (2, 1, 3):
            x = (xx + j) % 4
            start(
                remote(
                    summed.at[c, x], arrived.at[c, xx], g_s.at[c, j], g_r.at[c, xx], sp, 2 * x + core
                )
            )
        arrived[c, xx] = summed[c, xx]

    for c in range(n_chunk):
        cols = slice(c * piece, (c + 1) * piece)
        product = mm(mixed[...], wo[:, cols]).astype(bf16)
        for x in range(4):
            for k in range(2):
                lo = (2 * x + k) * own_n
                partial[c, k, x] = product[lo : lo + own_n]
        start(
            remote(
                partial.at[c, 1 - core], paired.at[c], o_s.at[c], o_r.at[c], sp, sibling
            )
        )
        if c >= lag:
            pass_on(c - lag)
    phase("wait_core")
    for c in range(n_chunk - lag, n_chunk):
        pass_on(c)
    phase("wait_x")
    pieces = []
    for c in range(n_chunk):
        for j in (1, 3, 2):
            x = (xx + j) % 4
            remote(
                summed.at[c, 0], arrived.at[c, x], g_s.at[c, j], g_r.at[c, x], sp, tp
            ).wait_recv()
        total = arrived[c, 0].astype(f32)
        for x in range(1, 4):
            total = total + arrived[c, x].astype(f32)
        pieces.append(total.astype(bf16).astype(f32))
    phase("final")
    square = sum(jnp.sum(p * p, axis=-1, keepdims=True) for p in pieces)
    inverse = lax.rsqrt(square * (1.0 / model) + NORM_EPS)
    for c in range(n_chunk):
        for s in range(piece // width):
            j = c * (piece // width) + s
            cols = slice(j * width, (j + 1) * width)
            value = pieces[c][:, s * width : (s + 1) * width]
            out[:, cols] = (
                own_rows[:, cols].astype(f32) + mods[j, 4:5] * (value * inverse)
            ).astype(bf16)

    phase("drain")
    for copy in sends:
        copy.wait_send()

    def drain_ctx(j, carry):
        remote(ctx_out.at[0], ctx_in.at[0], c_s.at[j], c_r.at[0], sp, tp).wait_send()
        return carry

    def drain(j, carry):
        remote(map_out.at[0], map_in.at[0], m_s.at[j], m_r.at[0], sp, tp).wait_send()
        remote(state_out.at[0], states.at[0], s_s.at[j], s_r.at[0], sp, tp).wait_send()
        return carry

    lax.fori_loop(0, N_SP, drain, 0)
    lax.fori_loop(1, N_SP, drain_ctx, 0)
    scopes.close()


def on_device(
    latent,
    context,
    condition,
    context_condition,
    shift_weight,
    scale_weight,
    gate_weight,
    norm_gain,
    decay_down,
    decay_up,
    rate_down,
    rate_up,
    head_bias,
    query_weight,
    key_weight,
    value_weight,
    branch_weight,
    group_gain,
    out_weight,
):
    own_n, model = latent.shape
    ctx_n = context.shape[0]
    width = query_weight.shape[1]
    held = condition.shape[0]
    args = (
        latent,
        context,
        condition.reshape(1, -1),
        context_condition.reshape(1, -1),
        shift_weight,
        scale_weight,
        gate_weight,
        norm_gain.reshape(1, -1),
        decay_down,
        decay_up,
        rate_down,
        rate_up,
        head_bias,
        query_weight,
        key_weight,
        value_weight,
        branch_weight,
        group_gain.reshape(1, -1),
        out_weight,
    )
    n_chunk = 8
    piece = model // n_chunk
    V = pltpu.VMEM
    dma = pltpu.SemaphoreType.DMA
    scratch = [
        V((N_TP, own_n, model), bf16),
        V((own_n, model), bf16),
        V((ctx_n, model), bf16),
        V((2, held), f32),
        V((3, held, width), bf16),
        V((1, model), f32),
        V((model, 2 * LEN), bf16),
        V((2, LEN, width), bf16),
        V((2, width), f32),
        V((model, width), bf16),
        V((model, width), bf16),
        V((model, width), bf16),
        V((model, width), bf16),
        V((1, width), f32),
        V((width, model), bf16),
        V((8, width), f32),
        V((4, 8, width), f32),
        V((8, width), f32),
        V((4, 8, width), f32),
        V((N_TP, 8, width), f32),
        V((LEN + ctx_n, model), bf16),
        V((LEN + ctx_n, 2 * LEN), bf16),
        V((LEN + ctx_n, width), bf16),
        V((LEN + ctx_n, width), bf16),
        V((LEN + ctx_n, width), bf16),
        V((LEN + ctx_n, width), bf16),
        V((LEN, width), bf16),
        V((LEN, width), bf16),
        V((8, ctx_n, 2 * LEN), bf16),
        V((N_SP, ctx_n, 2 * LEN), bf16),
        V((8, LEN), f32),
        V((N_SP, HALF, LEN), bf16),
        V((N_SP + 1, HALF, LEN), bf16),
        V((4, HALF, LEN), f32),
        V((width // LEN, 4, LEN, LEN), bf16),
        V((width // LEN, 2, 2 * LEN, LEN), bf16),
        V((width // LEN, 2, LEN, LEN), f32),
        V((width // LEN, 1, LEN), f32),
        V((width // LEN, LEN, 2 * LEN), bf16),
        V((width // LEN, LEN, LEN), f32),
        V((N_SP, HALF // 2, LEN), bf16),
        V((N_SP + 1, HALF // 2, LEN), bf16),
        V((LEN, width), bf16),
        V((n_chunk, 2, 4, own_n, piece), bf16),
        V((n_chunk, 4, own_n, piece), bf16),
        V((n_chunk, 4, own_n, piece), bf16),
        V((n_chunk, 4, own_n, piece), bf16),
        dma((19,)),
        dma((4,)),
        dma((4,)),
        dma((4,)),
        dma((4,)),
        dma((N_TP,)),
        dma((N_TP,)),
        dma((4,)),
        dma((N_TP,)),
        dma((4,)),
        dma((N_SP,)),
        dma((N_SP,)),
        dma((N_SP,)),
        dma((N_SP + 1,)),
        dma((N_SP,)),
        dma((N_SP + 1,)),
        dma((n_chunk,)),
        dma((n_chunk,)),
        dma((n_chunk, 4)),
        dma((n_chunk, 4)),
    ]
    return pl.pallas_call(
        kernel,
        out_shape=jax.ShapeDtypeStruct((own_n, model), bf16),
        in_specs=[pl.BlockSpec(memory_space=pl.ANY)] * len(args),
        out_specs=pl.BlockSpec(memory_space=pltpu.VMEM),
        scratch_shapes=scratch,
        compiler_params=pltpu.CompilerParams(
            collective_id=0, has_side_effects=True, vmem_limit_bytes=60 * 1024 * 1024
        ),
    )(*args)


def solution(mesh):
    placed = (
        P(("sp", "tp"), None),
        P("sp", None),
        P("sp"),
        P("sp"),
        P("sp", "tp"),
        P("sp", "tp"),
        P("sp", "tp"),
        P(),
        P(),
        P(None, "tp"),
        P(),
        P(None, "tp"),
        P(None, "tp"),
        P(None, "tp"),
        P(None, "tp"),
        P(None, "tp"),
        P(None, "tp"),
        P("tp"),
        P("tp", None),
    )
    return jax.shard_map(
        on_device, mesh=mesh, in_specs=placed, out_specs=P(("sp", "tp"), None), check_vma=False
    )
```

```python
import contextlib
import math

import jax
import jax.numpy as jnp
from jax import lax
from jax.experimental import pallas as pl
from jax.experimental.pallas import tpu as pltpu
from jax.sharding import PartitionSpec as P

HEAD_DIM = 64
NORM_EPS = 1e-06
GROUP_EPS = 0.00064
DECAY_TOP = math.exp(-0.5)
MESH = pl.DeviceIdType.MESH
bf16 = jnp.bfloat16
f32 = jnp.float32
LEN = 128
lag = 5
N_SP = 16
N_TP = 8
HALF = 64
FAR_FIRST = (
    (2, 2), (2, 1), (2, 3), (1, 2), (3, 2), (1, 1), (3, 3), (1, 3), (3, 1),
    (2, 0), (0, 2), (1, 0), (3, 0), (0, 1), (0, 3),
)
EVEN_FIRST = ((2, 2), (1, 2), (3, 2), (2, 0), (0, 2), (1, 0), (3, 0), (0, 0))
ODD_FIRST = ((2, 1), (2, 3), (1, 1), (3, 3), (1, 3), (3, 1), (0, 1), (0, 3))


def mm(a, b):
    return jnp.dot(a, b, preferred_element_type=f32)


def mm_nt(a, b):
    return lax.dot_general(a, b, (((1,), (1,)), ((), ())), preferred_element_type=f32)


def split(a):
    high = a.astype(bf16)
    return high, (a - high.astype(f32)).astype(bf16)


def rows_cols():
    row = lax.broadcasted_iota(jnp.int32, (LEN, LEN), 0)
    col = lax.broadcasted_iota(jnp.int32, (LEN, LEN), 1)
    return row, col


def cumulative(log_decay, row, col):
    lower = jnp.where(row >= col, 1.0, 0.0).astype(bf16)
    high, low = split(log_decay)
    return mm(lower, high) + mm(lower, low)


def solve(couplings, sides, cross):
    row, col = rows_cols()
    eye = jnp.where(row == col, 1.0, 0.0)
    inverse = [eye + jnp.where(cross == 1, a, 0.0) for a in couplings]
    size = 2
    while size < LEN // 2:
        level = (cross >= size) & (cross < 2 * size)
        low = [d.astype(bf16) for d in inverse]
        part = [mm(jnp.where(level, a, 0.0).astype(bf16), d) for a, d in zip(couplings, low)]
        inverse = [d + mm(e, p.astype(bf16)) for d, e, p in zip(inverse, low, part)]
        size *= 2
    level = (cross >= size) & (cross < 2 * size)
    low = [d.astype(bf16) for d in inverse]
    first = [mm(d, s.astype(bf16)) for d, s in zip(low, sides)]
    part = [
        mm(jnp.where(level, a, 0.0).astype(bf16), y.astype(bf16)) for a, y in zip(couplings, first)
    ]
    return [y + mm(d, p.astype(bf16)) for y, d, p in zip(first, low, part)]


def head_mask(head):
    lane = lax.broadcasted_iota(jnp.int32, (1, LEN), 1)
    return (lane >= HALF) if head else (lane < HALF)


def pair_unit(keys):
    own = head_mask(0)
    square = keys * keys
    sums = [
        jnp.sum(jnp.where(mask, square, 0.0), axis=-1, keepdims=True)
        for mask in (own, head_mask(1))
    ]
    return keys * lax.rsqrt(jnp.where(own, sums[0], sums[1]) + 1.0)


def state_map(transposed, solved, crossed, total, head):
    lo = head * HALF
    out = mm(
        transposed[lo : lo + HALF], jnp.concatenate([solved, crossed], axis=0)
    )
    row = lax.broadcasted_iota(jnp.int32, (HALF, LEN), 0)
    lane = lax.broadcasted_iota(jnp.int32, (HALF, LEN), 1)
    out = out + jnp.where(lane == row + lo, jnp.exp(total), 0.0)
    return pltpu.roll(out, HALF, 1) if head else out


def pair_setup(keys, values, log_decay, rate, row, col):
    cum = cumulative(log_decay, row, col)
    total = cum[LEN - 1 : LEN]
    half = 0.5 * total
    scale = jnp.exp(half)
    unit = pair_unit(keys)
    erase = -unit
    write = unit * rate
    before = jnp.exp(cum - log_decay - half)
    after = jnp.exp(half - cum)
    step = jnp.exp(log_decay)
    crossed_values = pltpu.roll(values, HALF, 1)
    fed_by = crossed_values.astype(bf16)
    own = [head_mask(0), head_mask(1)]
    units, rights, factors = [], [], []
    for direction in (0, 1):
        left, right = (before, after) if direction == 0 else (after, before)
        er = erase * left
        wr, kr = write * right, keys * right
        right_both = jnp.concatenate([wr, kr], axis=0).astype(bf16)
        rights.append(right_both)
        factors.append(left * step)
        transposed = jnp.concatenate(
            [jnp.transpose(wr * scale), jnp.transpose(kr * scale)], axis=1
        ).astype(bf16)
        left_both = jnp.concatenate([jnp.where(mask, er, 0.0) for mask in own], axis=0)
        grams = mm_nt(left_both.astype(bf16), right_both)
        strict = (row > col) if direction == 0 else (row < col)
        for head in (0, 1):
            rows = slice(head * LEN, (head + 1) * LEN)
            coupling = jnp.where(strict, grams[rows, :LEN], 0.0)
            feeding = jnp.where(strict, grams[rows, LEN:], 0.0).astype(bf16)
            side = jnp.where(own[head], er, mm(feeding, fed_by))
            units.append((coupling, side, transposed, head))
    return units, rights, factors, crossed_values, scale, total


def pairs_terms(inputs):
    row, col = rows_cols()
    setups = [pair_setup(*given, row, col) for given in inputs]
    flat = [unit for setup in setups for unit in setup[0]]
    answers = solve([u[0] for u in flat], [u[1] for u in flat], row ^ col)
    results, at = [], 0
    for units, rights, factors, crossed_values, scale, total in setups:
        maps, solved = [], []
        for _, _, transposed, head in units:
            mine = head_mask(head)
            answer = answers[at]
            at += 1
            rows = jnp.where(mine, answer * scale, answer).astype(bf16)
            crossed = jnp.where(mine, 0.0, crossed_values).astype(bf16)
            maps.append(state_map(transposed, rows, crossed, total, head))
            solved.append(rows)
        results.append((maps, solved, rights, factors, scale))
    return results


def pair_reads(queries, values, solved, rights, factors, scale):
    row, col = rows_cols()
    own = [head_mask(0), head_mask(1)]
    crossed_values = pltpu.roll(values, HALF, 1)
    crossed = [jnp.where(mask, 0.0, crossed_values).astype(bf16) for mask in own]
    reads = []
    for direction in (0, 1):
        qr = queries * factors[direction]
        left_both = jnp.concatenate([jnp.where(mask, qr, 0.0) for mask in own], axis=0)
        grams = mm_nt(left_both.astype(bf16), rights[direction])
        reach = (row >= col) if direction == 0 else (row <= col)
        both = jnp.concatenate([reach, reach], axis=1)
        for head in (0, 1):
            attend = jnp.where(both, grams[head * LEN : (head + 1) * LEN], 0.0).astype(bf16)
            reads.append(
                mm(attend, jnp.concatenate([solved[2 * direction + head], crossed[head]], axis=0))
                + jnp.where(own[head], qr * scale, 0.0)
            )
    ahead = [jnp.where(own[0], reads[at], reads[at + 1]) for at in (0, 2)]
    local = jnp.where(own[0], reads[1], reads[0]) + jnp.where(own[0], reads[3], reads[2])
    return jnp.concatenate(ahead, axis=1), pltpu.roll(local, HALF, 1)


def context_terms(pairs, lows, bias, backward):
    row, col = rows_cols()
    cross = row ^ col
    own = head_mask(0)
    order = (row - col) * (1 - 2 * backward)
    strict = order > 0
    units = []
    for pair, low in zip(pairs, lows):
        gates = jax.nn.sigmoid(bias + low)
        log_decay = jnp.where(own, -DECAY_TOP * gates, 0.0)
        rate = pltpu.roll(gates, HALF, 1)
        keys = jnp.where(own, pair, 0.0)
        cum = cumulative(log_decay, row, col)
        total = cum[LEN - 1 : LEN]
        half = 0.5 * total
        scale = jnp.exp(half)
        unit = keys * lax.rsqrt(jnp.sum(keys * keys, axis=-1, keepdims=True) + 1.0)
        one, two = cum - log_decay - half, half - cum
        left = jnp.exp(jnp.where(backward == 0, one, two))
        right = jnp.exp(jnp.where(backward == 0, two, one))
        er, wr, kr = -unit * left, unit * rate * right, keys * right
        grams = mm_nt(er.astype(bf16), jnp.concatenate([wr, kr], axis=0).astype(bf16))
        coupling = jnp.where(strict, grams[:, :LEN], 0.0)
        feeding = jnp.where(strict, grams[:, LEN:], 0.0).astype(bf16)
        crossed = jnp.where(own, 0.0, pair).astype(bf16)
        side = jnp.where(own, er, mm(feeding, crossed))
        transposed = jnp.concatenate(
            [jnp.transpose(wr * scale), jnp.transpose(kr * scale)], axis=1
        ).astype(bf16)
        units.append((coupling, side, transposed, crossed, scale, total))
    answers = solve([u[0] for u in units], [u[1] for u in units], cross)
    maps = []
    for (_, _, transposed, crossed, scale, total), answer in zip(units, answers):
        solved = jnp.where(own, answer * scale, answer).astype(bf16)
        maps.append(state_map(transposed, solved, crossed, total, 0))
    return maps


def compose(earlier, later):
    high, low = split(earlier)
    transfer = later[:, :HALF].astype(bf16)
    lane = lax.broadcasted_iota(jnp.int32, (1, LEN), 1)
    return mm(transfer, high) + mm(transfer, low) + jnp.where(lane >= HALF, later, 0.0)


def remote(src, dst, send, recv, sp, tp):
    return pltpu.make_async_remote_copy(
        src_ref=src,
        dst_ref=dst,
        send_sem=send,
        recv_sem=recv,
        device_id=(sp, tp),
        device_id_type=MESH,
    )


def kernel(
    latent,
    context,
    condition,
    context_condition,
    shift_weight,
    scale_weight,
    gate_weight,
    norm_gain,
    decay_down,
    decay_up,
    rate_down,
    rate_up,
    head_bias,
    query_weight,
    key_weight,
    value_weight,
    branch_weight,
    group_gain,
    out_weight,
    out,
    rows,
    own_rows,
    ctx_rows,
    cond,
    mod_w,
    gain,
    down,
    up,
    bias,
    wq,
    wk,
    wv,
    wb,
    ggain,
    wo,
    part,
    ybuf,
    zpart,
    zbuf,
    mods,
    gpart,
    gbuf,
    gsum,
    gmods,
    normed,
    low,
    kbuf,
    vbuf,
    dbuf,
    rbuf,
    qbuf,
    bbuf,
    ctx_out,
    ctx_in,
    head_rows,
    map_out,
    map_in,
    ctx_maps,
    solved_buf,
    right_buf,
    factor_buf,
    scale_buf,
    ahead,
    local,
    state_out,
    states,
    mixed,
    partial,
    paired,
    summed,
    arrived,
    load,
    y_s,
    y_r,
    z_s,
    z_r,
    t_s,
    t_r,
    l_s,
    l_r,
    f_s,
    c_s,
    c_r,
    m_s,
    m_r,
    s_s,
    s_r,
    o_s,
    o_r,
    g_s,
    g_r,
    gs_s,
    gs_r,
    gt_s,
    gt_r,
):
    sp = lax.axis_index("sp")
    tp = lax.axis_index("tp")
    zz, yy = sp // 4, sp % 4
    xx, core = tp // 2, tp % 2
    sibling = 2 * xx + (1 - core)

    def at_offset(dz, dy):
        return ((zz + dz) % 4) * 4 + (yy + dy) % 4

    width = wq.shape[1]
    model = normed.shape[1]
    blocks = model // width
    own_n = own_rows.shape[0]
    ctx_n = ctx_rows.shape[0]

    scopes = contextlib.ExitStack()

    def phase(name):
        scopes.close()
        scopes.enter_context(jax.named_scope(name))

    phase("greet")
    barrier = pltpu.get_barrier_semaphore()

    for j in (2, 1, 3):
        for to in (zz * 4 + (yy + j) % 4, ((zz + j) % 4) * 4 + yy):
            pl.semaphore_signal(barrier, inc=1, device_id=(to, tp), device_id_type=MESH)
    for j in range(1, N_TP):
        pl.semaphore_signal(
            barrier, inc=1, device_id=(sp, (tp + j) % N_TP), device_id_type=MESH
        )

    def fetch(at, src, dst):
        return pltpu.make_async_copy(src, dst, load.at[at])

    copies = [
        fetch(0, condition, cond.at[0:1]),
        fetch(1, context_condition, cond.at[1:2]),
        fetch(2, shift_weight, mod_w.at[0]),
        fetch(3, scale_weight, mod_w.at[1]),
        fetch(4, gate_weight, mod_w.at[2]),
        fetch(6, context, ctx_rows),
        fetch(7, norm_gain, gain),
        fetch(8, decay_down, down.at[:, 0:LEN]),
        fetch(9, rate_down, down.at[:, LEN : 2 * LEN]),
        fetch(10, decay_up, up.at[0]),
        fetch(11, rate_up, up.at[1]),
        fetch(12, head_bias, bias),
        fetch(13, key_weight, wk),
        fetch(14, value_weight, wv),
        fetch(15, query_weight, wq),
        fetch(16, branch_weight, wb),
        fetch(17, group_gain, ggain),
        fetch(18, out_weight, wo),
    ]
    copies.insert(5, fetch(5, latent, own_rows))
    copies[5].start()
    for copy in copies[:5] + copies[6:]:
        copy.start()

    phase("barrier")
    copies[5].wait()
    pl.semaphore_wait(barrier, 6 + N_TP - 1)
    sends = []

    def start(copy):
        copy.start()
        sends.append(copy)

    for j in (2, 1, 3):
        to = 2 * ((xx + j) % 4) + core
        start(remote(own_rows, rows.at[tp], l_s.at[j], l_r.at[tp], sp, to))
    start(remote(own_rows, rows.at[tp], l_s.at[0], l_r.at[tp], sp, sibling))
    rows[tp] = own_rows[...]

    phase("wait_mod_w")
    for at in (0, 1, 2, 3, 4):
        copies[at].wait()
    phase("shares")
    rows_c = cond[...]
    conditions = (rows_c * jax.nn.sigmoid(rows_c)).astype(bf16)
    conditions = jnp.concatenate([conditions, jnp.zeros((14, rows_c.shape[1]), bf16)], axis=0)
    shares = [mm(conditions, mod_w[at]) for at in range(3)]
    halves = (slice(0, width // 2), slice(width // 2, width))
    part[...] = jnp.concatenate(
        [share[0:2, half] for half in halves for share in shares[:2]], axis=0
    )
    gpart[...] = jnp.concatenate(
        [shares[2][0:1, k * LEN : (k + 1) * LEN] for k in range(width // LEN)]
        + [jnp.zeros((8 - width // LEN, LEN), f32)],
        axis=0,
    )
    ybuf[yy] = part[...]
    gbuf[0, yy] = gpart[...]
    phase("send_y")
    for j in (2, 1, 3):
        to = zz * 4 + (yy + j) % 4
        start(remote(part, ybuf.at[yy], y_s.at[j], y_r.at[yy], to, tp))
    for j in (1, 2, 3):
        to = zz * 4 + (yy + j) % 4
        start(remote(gpart, gbuf.at[0, yy], gs_s.at[0, j], gs_r.at[0, yy], to, tp))
    phase("wait_y")
    for j in (1, 2, 3):
        frm = (yy + j) % 4
        remote(part, ybuf.at[frm], y_s.at[j], y_r.at[frm], sp, tp).wait_recv()
    zpart[...] = ybuf[0] + ybuf[1] + ybuf[2] + ybuf[3]
    zbuf[zz] = zpart[...]
    for j in (2, 1, 3):
        to = ((zz + j) % 4) * 4 + yy
        start(remote(zpart, zbuf.at[zz], z_s.at[j], z_r.at[zz], to, tp))

    phase("ctx_stats")
    copies[6].wait()
    ctx = ctx_rows[...].astype(f32)
    ctx_scale = lax.rsqrt(jnp.mean(ctx * ctx, axis=-1, keepdims=True) + NORM_EPS)

    phase("wait_z")
    for j in (1, 2, 3):
        frm = (zz + j) % 4
        remote(zpart, zbuf.at[frm], z_s.at[j], z_r.at[frm], sp, tp).wait_recv()
    part2 = zbuf[0] + zbuf[1] + zbuf[2] + zbuf[3]
    mods[tp] = part2
    for j in (4, 5, 2, 3, 6, 7, 1):
        to = 2 * ((xx + j // 2) % 4) + (core + j) % 2
        start(remote(mods.at[tp], mods.at[tp], t_s.at[j], t_r.at[tp], sp, to))

    phase("latent_x")
    for j in (1, 3, 2):
        frm = 2 * ((xx + j) % 4) + core
        remote(own_rows, rows.at[frm], l_s.at[j], l_r.at[frm], sp, tp).wait_recv()
        start(remote(rows.at[frm], rows.at[frm], f_s.at[j], l_r.at[frm], sp, sibling))
    phase("latent_core")
    for j in (0, 1, 3, 2):
        frm = 2 * ((xx + j) % 4) + (1 - core)
        remote(own_rows, rows.at[frm], l_s.at[j], l_r.at[frm], sp, tp).wait_recv()
    phase("latent_stats")
    inverses = []
    for i in range(N_TP):
        values = rows[i].astype(f32)
        inverses.append(lax.rsqrt(jnp.mean(values * values, axis=-1, keepdims=True) + NORM_EPS))

    phase("wait_t")
    copies[7].wait()
    for j in range(1, N_TP):
        frm = (tp + j) % N_TP
        remote(part, mods.at[frm], t_s.at[j], t_r.at[frm], sp, tp).wait_recv()

    phase("normalize")
    for j in range(2 * blocks):
        cols = slice(j * width // 2, (j + 1) * width // 2)
        vectors = mods[j // 2, 4 * (j % 2) : 4 * (j % 2) + 4]
        factor = gain[0:1, cols] * (1.0 + vectors[2:3])
        shift = vectors[0:1]
        for i in range(N_TP):
            normed[i * own_n : (i + 1) * own_n, cols] = (
                rows[i, :, cols].astype(f32) * inverses[i] * factor + shift
            ).astype(bf16)
        factor = gain[0:1, cols] * (1.0 + vectors[3:4])
        shift = vectors[1:2]
        normed[LEN : LEN + ctx_n, cols] = (
            ctx_rows[:, cols].astype(f32) * ctx_scale * factor + shift
        ).astype(bf16)

    for j in (1, 2, 3):
        frm = (yy + j) % 4
        remote(gpart, gbuf.at[0, frm], gs_s.at[0, j], gs_r.at[0, frm], sp, tp).wait_recv()
    gsum[0] = gbuf[0, 0] + gbuf[0, 1] + gbuf[0, 2] + gbuf[0, 3]
    gbuf[1, zz] = gsum[0]
    for j in (1, 2, 3):
        to = ((zz + j) % 4) * 4 + yy
        start(remote(gsum.at[0], gbuf.at[1, zz], gs_s.at[1, j], gs_r.at[1, zz], to, tp))

    phase("lows")
    for at in (8, 9, 10, 11, 12):
        copies[at].wait()
    lows = mm(normed[...], down[...])
    low[:, :LEN] = jnp.tanh(lows[:, :LEN]).astype(bf16)
    low[:, LEN:] = lows[:, LEN:].astype(bf16)
    dbuf[...] = mm(low[:, :LEN], up[0]).astype(bf16)
    rbuf[...] = mm(low[:, LEN:], up[1]).astype(bf16)

    def project(weight, to, count):
        def body(i, carry):
            at = pl.ds(pl.multiple_of(i * 256, 256), 256)
            to[:, at] = mm(normed[0:count], weight[:, at]).astype(bf16)
            return carry

        lax.fori_loop(0, width // 256, body, 0)

    phase("proj_kv")
    copies[13].wait()
    project(wk, kbuf, LEN + ctx_n)
    copies[14].wait()
    project(wv, vbuf, LEN + ctx_n)

    phase("ctx_pack")
    lane = lax.broadcasted_iota(jnp.int32, (1, LEN), 1)
    left = lane < HALF
    for p in range(width // LEN):
        cols = slice(p * LEN, (p + 1) * LEN)
        for at, (first, second) in enumerate(((kbuf, vbuf), (dbuf, rbuf))):
            a = first[LEN : LEN + ctx_n, cols].astype(f32)
            b = second[LEN : LEN + ctx_n, cols].astype(f32)
            lanes = slice(at * LEN, (at + 1) * LEN)
            ctx_out[2 * p, :, lanes] = jnp.where(left, a, pltpu.roll(b, HALF, 1)).astype(bf16)
            ctx_out[2 * p + 1, :, lanes] = jnp.where(left, pltpu.roll(a, HALF, 1), b).astype(bf16)
        a = bias[0:1, cols]
        b = bias[1:2, cols]
        head_rows[2 * p : 2 * p + 1] = jnp.where(left, a, pltpu.roll(b, HALF, 1))
        head_rows[2 * p + 1 : 2 * p + 2] = jnp.where(left, pltpu.roll(a, HALF, 1), b)
    my_head = sp % 8
    backward = sp // 8
    ctx_in[sp] = ctx_out[my_head]

    for dz, dy in FAR_FIRST:
        to = at_offset(dz, dy)
        start(
            remote(
                ctx_out.at[to % 8], ctx_in.at[sp], c_s.at[4 * dz + dy], c_r.at[sp], to, tp
            )
        )

    phase("chunks")
    def place(to):
        slot = jnp.where(to == sp, N_SP, sp)
        return slot, jnp.where(to == sp, sibling, tp)

    def chunk():
        inputs, at = [], []
        for k in range(width // LEN):
            p = k
            cols = slice(p * LEN, (p + 1) * LEN)
            gates = jax.nn.sigmoid(bias[0:1, cols] + dbuf[0:LEN, cols].astype(f32))
            rate = jax.nn.sigmoid(bias[1:2, cols] + rbuf[0:LEN, cols].astype(f32))
            inputs.append(
                (
                    kbuf[0:LEN, cols].astype(f32),
                    vbuf[0:LEN, cols].astype(f32),
                    -DECAY_TOP * gates,
                    rate,
                )
            )
            at.append(p)
        found = pairs_terms(inputs)
        for p, (maps, solved, rights, factors, scale) in zip(at, found):
            for direction in (0, 1):
                for head in (0, 1):
                    map_out[direction * 8 + 2 * p + head] = maps[2 * direction + head].astype(bf16)
        for dz, dy in FAR_FIRST:
            to = at_offset(dz, dy)
            start(remote(map_out.at[to], map_in.at[sp], m_s.at[to], m_r.at[sp], to, tp))
        for p, (maps, solved, rights, factors, scale) in zip(at, found):
            for direction in (0, 1):
                for head in (0, 1):
                    solved_buf[p, 2 * direction + head] = solved[2 * direction + head]
                right_buf[p, direction] = rights[direction]
                factor_buf[p, direction] = factors[direction]
            scale_buf[p] = scale

    chunk()
    map_in[sp] = map_out[sp]

    for j in (1, 2, 3):
        frm = (zz + j) % 4
        remote(gpart, gbuf.at[1, frm], gs_s.at[1, j], gs_r.at[1, frm], sp, tp).wait_recv()
    gmods[tp] = gbuf[1, 0] + gbuf[1, 1] + gbuf[1, 2] + gbuf[1, 3]
    for j in range(1, N_TP):
        to = (tp + j) % N_TP
        start(remote(gmods.at[tp], gmods.at[tp], gt_s.at[j], gt_r.at[tp], sp, to))

    phase("wait_ctx")
    for j in range(1, N_SP):
        frm = (sp + j) % N_SP
        remote(ctx_out.at[0], ctx_in.at[frm], c_s.at[j], c_r.at[frm], sp, tp).wait_recv()
    phase("ctx_chunks")
    my_bias = head_rows[pl.ds(my_head, 1)]
    per = LEN // ctx_n
    pairs, lows_in = [], []
    for c in range(N_SP // per):
        pairs.append(ctx_in[c * per : (c + 1) * per, :, 0:LEN].astype(f32).reshape(LEN, LEN))
        lows_in.append(ctx_in[c * per : (c + 1) * per, :, LEN:].astype(f32).reshape(LEN, LEN))
    for c, found in enumerate(context_terms(pairs, lows_in, my_bias, backward)):
        ctx_maps[c] = found
    phase("proj_b")
    copies[16].wait()
    project(wb, bbuf, LEN)
    phase("wait_maps")
    for copy in sends:
        copy.wait_send()
    drained = len(sends)
    for j in range(1, N_SP):
        frm = (sp + j) % N_SP
        remote(map_out.at[0], map_in.at[frm], m_s.at[0], m_r.at[frm], sp, tp).wait_recv()
    phase("walk")
    count = N_SP // per
    forward = backward == 0
    order = [jnp.where(forward, i, N_SP - 1 - i) for i in range(N_SP)]
    steps = [map_in[order[i]].astype(f32) for i in range(N_SP - 1)]
    state = ctx_maps[jnp.where(forward, 0, count - 1)]
    for c in range(1, count):
        state = compose(state, ctx_maps[jnp.where(forward, c, count - 1 - c)])
    two = [compose(steps[2 * i], steps[2 * i + 1]) for i in range(7)]
    four = [compose(two[2 * i], two[2 * i + 1]) for i in range(3)]
    eight = compose(four[0], four[1])
    odd = my_head % 2
    left = lax.broadcasted_iota(jnp.int32, (1, LEN), 1) < HALF

    def show(i, state):
        to = order[i]
        state_out[to] = jnp.where(
            left, pltpu.roll(state[: HALF // 2], HALF, 1), state[HALF // 2 :]
        ).astype(bf16)

    def launch(to):
        slot, over = place(to)
        remote(state_out.at[to], states.at[slot], s_s.at[to], s_r.at[slot], to, over).start()

    held = {0: state}
    show(0, state)
    held[8] = compose(state, eight)
    held[4] = compose(state, four[0])
    show(8, held[8])
    show(4, held[4])
    for i in (0, 8, 4):
        launch(order[i])
    held[12] = compose(held[8], four[2])
    held[2] = compose(state, two[0])
    held[6] = compose(held[4], two[2])
    held[10] = compose(held[8], two[4])
    held[14] = compose(held[12], two[6])
    for i in (2, 6, 10, 12, 14):
        show(i, held[i])
    for i in (2, 6, 10, 12, 14):
        launch(order[i])
    for i in range(1, N_SP, 2):
        show(i, compose(held[i - 1], steps[i - 1]))
    even = (yy % 2 == 0) == (backward == 1)
    for one, other in zip(EVEN_FIRST, ODD_FIRST):
        launch(jnp.where(even, at_offset(*one), at_offset(*other)))
    states[sp] = state_out[sp]

    phase("proj_qb")
    copies[15].wait()
    project(wq, qbuf, LEN)
    phase("read_terms")

    def read_terms(p, carry):
        cols = pl.ds(pl.multiple_of(p * LEN, LEN), LEN)
        coming, here = pair_reads(
            qbuf[:, cols].astype(f32),
            vbuf[0:LEN, cols].astype(f32),
            [solved_buf[p, i] for i in range(4)],
            [right_buf[p, i] for i in range(2)],
            [factor_buf[p, i] for i in range(2)],
            scale_buf[p],
        )
        ahead[p] = coming.astype(bf16)
        local[p] = here
        return carry

    lax.fori_loop(0, width // LEN, read_terms, 0)

    phase("wait_states")
    for j in range(1, N_SP + 1):
        frm = (sp + j) % N_SP if j < N_SP else N_SP
        remote(state_out.at[0], states.at[frm], s_s.at[0], s_r.at[frm], sp, tp).wait_recv()

    phase("reads")
    for j in range(1, N_TP):
        frm = (tp + j) % N_TP
        remote(gpart, gmods.at[frm], gt_s.at[j], gt_r.at[frm], sp, tp).wait_recv()
    copies[17].wait()
    other = lane >= HALF
    for p in range(width // LEN):
        cols = slice(p * LEN, (p + 1) * LEN)
        blocks_in = []
        for at in (2 * p, 8 + 2 * p):
            first, second = states[at].astype(f32), states[at + 1].astype(f32)
            blocks_in += [
                jnp.where(left, first, 0.0),
                jnp.where(left, pltpu.roll(first, HALF, 1), 0.0),
                jnp.where(left, 0.0, pltpu.roll(second, HALF, 1)),
                jnp.where(left, 0.0, second),
            ]
        both = jnp.concatenate(blocks_in, axis=0).astype(bf16)
        reads = mm(ahead[p], both) + local[p]

        def head_mean(x):
            sums = [
                jnp.sum(jnp.where(mask, x, 0.0), axis=-1, keepdims=True) for mask in (left, other)
            ]
            return jnp.where(left, sums[0], sums[1]) * (1.0 / HALF)

        centred = reads - head_mean(reads)
        normal = centred * lax.rsqrt(head_mean(centred * centred) + GROUP_EPS)
        gate = bbuf[:, cols].astype(f32)
        mixed[:, cols] = (
            normal * ggain[0:1, cols] * (gate * jax.nn.sigmoid(gate))
        ).astype(bf16)

    phase("out_proj")
    copies[18].wait()
    n_chunk = arrived.shape[0]
    piece = model // n_chunk

    def chip_sum(c, x):
        return partial[c, core, x].astype(f32) + paired[c, x].astype(f32)

    def send_x(c, j):
        x = (xx + j) % 4
        start(
            remote(
                summed.at[c, j - 1], arrived.at[c, j - 1], g_s.at[c, j - 1], g_r.at[c, j - 1], sp,
                2 * x + core,
            )
        )

    def pass_on(c):
        remote(partial.at[c, 0], paired.at[c], o_s.at[c], o_r.at[c], sp, tp).wait_recv()
        for j in (2, 1, 3):
            summed[c, j - 1] = chip_sum(c, (xx + j) % 4).astype(bf16)
        send_x(c, 2)
        if c % 2 == 1:
            for at in (c - 1, c):
                send_x(at, 1)
                send_x(at, 3)

    for c in range(n_chunk):
        cols = slice(c * piece, (c + 1) * piece)
        product = mm(mixed[...], wo[:, cols]).astype(bf16)
        for x in range(4):
            for k in range(2):
                lo = (2 * x + k) * own_n
                partial[c, k, x] = product[lo : lo + own_n]
        start(
            remote(
                partial.at[c, 1 - core], paired.at[c], o_s.at[c], o_r.at[c], sp, sibling
            )
        )
        if c >= lag:
            pass_on(c - lag)
    phase("wait_core")
    for c in range(n_chunk - lag, n_chunk):
        pass_on(c)
    phase("wait_x")
    pieces = []
    for c in range(n_chunk):
        for k in (0, 2, 1):
            remote(
                summed.at[c, 0], arrived.at[c, k], g_s.at[c, k], g_r.at[c, k], sp, tp
            ).wait_recv()
        total = chip_sum(c, xx)
        for k in range(3):
            total = total + arrived[c, k].astype(f32)
        pieces.append(total.astype(bf16).astype(f32))
    phase("final")
    square = sum(jnp.sum(p * p, axis=-1, keepdims=True) for p in pieces)
    inverse = lax.rsqrt(square * (1.0 / model) + NORM_EPS)
    for c in range(n_chunk):
        for k in range(piece // LEN):
            lo = c * piece + k * LEN
            cols = slice(lo, lo + LEN)
            lane_block = lo // LEN
            per_tp = width // LEN
            gate = gmods[lane_block // per_tp, lane_block % per_tp : lane_block % per_tp + 1]
            value = pieces[c][:, k * LEN : (k + 1) * LEN]
            out[:, cols] = (own_rows[:, cols].astype(f32) + gate * (value * inverse)).astype(bf16)

    phase("drain")
    for copy in sends[drained:]:
        copy.wait_send()

    for j in range(N_SP):
        remote(state_out.at[0], states.at[0], s_s.at[j], s_r.at[0], sp, tp).wait_send()
    scopes.close()


def on_device(
    latent,
    context,
    condition,
    context_condition,
    shift_weight,
    scale_weight,
    gate_weight,
    norm_gain,
    decay_down,
    decay_up,
    rate_down,
    rate_up,
    head_bias,
    query_weight,
    key_weight,
    value_weight,
    branch_weight,
    group_gain,
    out_weight,
):
    own_n, model = latent.shape
    ctx_n = context.shape[0]
    width = query_weight.shape[1]
    held = condition.shape[0]
    args = (
        latent,
        context,
        condition.reshape(1, -1),
        context_condition.reshape(1, -1),
        shift_weight,
        scale_weight,
        gate_weight,
        norm_gain.reshape(1, -1),
        decay_down,
        decay_up,
        rate_down,
        rate_up,
        head_bias,
        query_weight,
        key_weight,
        value_weight,
        branch_weight,
        group_gain.reshape(1, -1),
        out_weight,
    )
    n_chunk = 8
    piece = model // n_chunk
    V = pltpu.VMEM
    dma = pltpu.SemaphoreType.DMA
    scratch = [
        V((N_TP, own_n, model), bf16),
        V((own_n, model), bf16),
        V((ctx_n, model), bf16),
        V((2, held), f32),
        V((3, held, width), bf16),
        V((1, model), f32),
        V((model, 2 * LEN), bf16),
        V((2, LEN, width), bf16),
        V((2, width), f32),
        V((model, width), bf16),
        V((model, width), bf16),
        V((model, width), bf16),
        V((model, width), bf16),
        V((1, width), f32),
        V((width, model), bf16),
        V((8, width // 2), f32),
        V((4, 8, width // 2), f32),
        V((8, width // 2), f32),
        V((4, 8, width // 2), f32),
        V((N_TP, 8, width // 2), f32),
        V((8, LEN), f32),
        V((2, 4, 8, LEN), f32),
        V((1, 8, LEN), f32),
        V((N_TP, 8, LEN), f32),
        V((LEN + ctx_n, model), bf16),
        V((LEN + ctx_n, 2 * LEN), bf16),
        V((LEN + ctx_n, width), bf16),
        V((LEN + ctx_n, width), bf16),
        V((LEN + ctx_n, width), bf16),
        V((LEN + ctx_n, width), bf16),
        V((LEN, width), bf16),
        V((LEN, width), bf16),
        V((8, ctx_n, 2 * LEN), bf16),
        V((N_SP, ctx_n, 2 * LEN), bf16),
        V((8, LEN), f32),
        V((N_SP, HALF, LEN), bf16),
        V((N_SP + 1, HALF, LEN), bf16),
        V((4, HALF, LEN), f32),
        V((width // LEN, 4, LEN, LEN), bf16),
        V((width // LEN, 2, 2 * LEN, LEN), bf16),
        V((width // LEN, 2, LEN, LEN), f32),
        V((width // LEN, 1, LEN), f32),
        V((width // LEN, LEN, 2 * LEN), bf16),
        V((width // LEN, LEN, LEN), f32),
        V((N_SP, HALF // 2, LEN), bf16),
        V((N_SP + 1, HALF // 2, LEN), bf16),
        V((LEN, width), bf16),
        V((n_chunk, 2, 4, own_n, piece), bf16),
        V((n_chunk, 4, own_n, piece), bf16),
        V((n_chunk, 3, own_n, piece), bf16),
        V((n_chunk, 3, own_n, piece), bf16),
        dma((19,)),
        dma((4,)),
        dma((4,)),
        dma((4,)),
        dma((4,)),
        dma((N_TP,)),
        dma((N_TP,)),
        dma((4,)),
        dma((N_TP,)),
        dma((4,)),
        dma((N_SP,)),
        dma((N_SP,)),
        dma((N_SP,)),
        dma((N_SP + 1,)),
        dma((N_SP,)),
        dma((N_SP + 1,)),
        dma((n_chunk,)),
        dma((n_chunk,)),
        dma((n_chunk, 3)),
        dma((n_chunk, 3)),
        dma((2, 4)),
        dma((2, 4)),
        dma((N_TP,)),
        dma((N_TP,)),
    ]
    return pl.pallas_call(
        kernel,
        out_shape=jax.ShapeDtypeStruct((own_n, model), bf16),
        in_specs=[pl.BlockSpec(memory_space=pl.ANY)] * len(args),
        out_specs=pl.BlockSpec(memory_space=pltpu.VMEM),
        scratch_shapes=scratch,
        compiler_params=pltpu.CompilerParams(
            collective_id=0, has_side_effects=True, vmem_limit_bytes=60 * 1024 * 1024
        ),
    )(*args)


def solution(mesh):
    placed = (
        P(("sp", "tp"), None),
        P("sp", None),
        P("sp"),
        P("sp"),
        P("sp", "tp"),
        P("sp", "tp"),
        P("sp", "tp"),
        P(),
        P(),
        P(None, "tp"),
        P(),
        P(None, "tp"),
        P(None, "tp"),
        P(None, "tp"),
        P(None, "tp"),
        P(None, "tp"),
        P(None, "tp"),
        P("tp"),
        P("tp", None),
    )
    return jax.shard_map(
        on_device, mesh=mesh, in_specs=placed, out_specs=P(("sp", "tp"), None), check_vma=False
    )
```

```python
import contextlib
import math

import jax
import jax.numpy as jnp
from jax import lax
from jax.experimental import pallas as pl
from jax.experimental.pallas import tpu as pltpu
from jax.sharding import PartitionSpec as P

HEAD_DIM = 64
NORM_EPS = 1e-06
GROUP_EPS = 0.00064
DECAY_TOP = math.exp(-0.5)
MESH = pl.DeviceIdType.MESH
bf16 = jnp.bfloat16
f32 = jnp.float32
LEN = 128
lag = 5
N_SP = 16
N_TP = 8
HALF = 64
FAR_FIRST = (
    (2, 2), (2, 1), (2, 3), (1, 2), (3, 2), (1, 1), (3, 3), (1, 3), (3, 1),
    (2, 0), (0, 2), (1, 0), (3, 0), (0, 1), (0, 3),
)
EVEN_FIRST = ((2, 2), (1, 2), (3, 2), (2, 0), (0, 2), (1, 0), (3, 0), (0, 0))
ODD_FIRST = ((2, 1), (2, 3), (1, 1), (3, 3), (1, 3), (3, 1), (0, 1), (0, 3))


def mm(a, b):
    return jnp.dot(a, b, preferred_element_type=f32)


def mm_nt(a, b):
    return lax.dot_general(a, b, (((1,), (1,)), ((), ())), preferred_element_type=f32)


def split(a):
    high = a.astype(bf16)
    return high, (a - high.astype(f32)).astype(bf16)


def rows_cols():
    row = lax.broadcasted_iota(jnp.int32, (LEN, LEN), 0)
    col = lax.broadcasted_iota(jnp.int32, (LEN, LEN), 1)
    return row, col


def cumulative(log_decay, row, col):
    lower = jnp.where(row >= col, 1.0, 0.0).astype(bf16)
    high, low = split(log_decay)
    return mm(lower, high) + mm(lower, low)


def solve(couplings, sides, cross):
    row, col = rows_cols()
    eye = jnp.where(row == col, 1.0, 0.0)
    inverse = [eye + jnp.where(cross == 1, a, 0.0) for a in couplings]
    size = 2
    while size < LEN // 2:
        level = (cross >= size) & (cross < 2 * size)
        low = [d.astype(bf16) for d in inverse]
        part = [mm(jnp.where(level, a, 0.0).astype(bf16), d) for a, d in zip(couplings, low)]
        inverse = [d + mm(e, p.astype(bf16)) for d, e, p in zip(inverse, low, part)]
        size *= 2
    level = (cross >= size) & (cross < 2 * size)
    low = [d.astype(bf16) for d in inverse]
    first = [mm(d, s.astype(bf16)) for d, s in zip(low, sides)]
    part = [
        mm(jnp.where(level, a, 0.0).astype(bf16), y.astype(bf16)) for a, y in zip(couplings, first)
    ]
    return [y + mm(d, p.astype(bf16)) for y, d, p in zip(first, low, part)]


def solve_both(couplings, sides, row, col):
    cross = row ^ col
    lower, upper = row >= col, row <= col
    eye = jnp.where(row == col, 1.0, 0.0)
    held = [eye + jnp.where(cross == 1, a, 0.0) for a in couplings]
    size = 2
    while size < LEN // 2:
        late = (row & size) != 0
        level = (cross >= size) & (cross < 2 * size)
        inner = (late & upper) | (~late & lower)
        outer = (late & lower) | (~late & upper)
        part = [
            mm(jnp.where(level, a, 0.0).astype(bf16), jnp.where(inner, h, 0.0).astype(bf16))
            for a, h in zip(couplings, held)
        ]
        held = [
            h + mm(jnp.where(outer, h, 0.0).astype(bf16), p.astype(bf16))
            for h, p in zip(held, part)
        ]
        size *= 2
    late = (row & size) != 0
    level = (cross >= size) & (cross < 2 * size)
    outer = (late & lower) | (~late & upper)
    first = [
        (
            mm(jnp.where(lower, h, 0.0).astype(bf16), f.astype(bf16)),
            mm(jnp.where(upper, h, 0.0).astype(bf16), b.astype(bf16)),
        )
        for h, (f, b) in zip(held, sides)
    ]
    part = [
        mm(jnp.where(level, a, 0.0).astype(bf16), jnp.where(late, b, f).astype(bf16))
        for a, (f, b) in zip(couplings, first)
    ]
    last = [
        mm(jnp.where(outer, h, 0.0).astype(bf16), p.astype(bf16)) for h, p in zip(held, part)
    ]
    return [
        (f + jnp.where(late, u, 0.0), b + jnp.where(late, 0.0, u))
        for (f, b), u in zip(first, last)
    ]


def head_mask(head):
    lane = lax.broadcasted_iota(jnp.int32, (1, LEN), 1)
    return (lane >= HALF) if head else (lane < HALF)


def pair_unit(keys):
    own = head_mask(0)
    square = keys * keys
    sums = [
        jnp.sum(jnp.where(mask, square, 0.0), axis=-1, keepdims=True)
        for mask in (own, head_mask(1))
    ]
    return keys * lax.rsqrt(jnp.where(own, sums[0], sums[1]) + 1.0)


def state_map(transposed, solved, crossed, total, head):
    lo = head * HALF
    out = mm(
        transposed[lo : lo + HALF], jnp.concatenate([solved, crossed], axis=0)
    )
    row = lax.broadcasted_iota(jnp.int32, (HALF, LEN), 0)
    lane = lax.broadcasted_iota(jnp.int32, (HALF, LEN), 1)
    out = out + jnp.where(lane == row + lo, jnp.exp(total), 0.0)
    return pltpu.roll(out, HALF, 1) if head else out


def pair_setup(keys, values, log_decay, rate, row, col):
    cum = cumulative(log_decay, row, col)
    total = cum[LEN - 1 : LEN]
    half = 0.5 * total
    scale = jnp.exp(half)
    unit = pair_unit(keys)
    erase = -unit
    write = unit * rate
    before = jnp.exp(cum - log_decay - half)
    after = jnp.exp(half - cum)
    step = jnp.exp(log_decay)
    crossed_values = pltpu.roll(values, HALF, 1)
    fed_by = crossed_values.astype(bf16)
    own = [head_mask(0), head_mask(1)]
    couplings, sides, rights, factors, transposes = [], [], [], [], []
    for direction in (0, 1):
        left, right = (before, after) if direction == 0 else (after, before)
        er = erase * left
        wr, kr = write * right, keys * right
        right_both = jnp.concatenate([wr, kr], axis=0).astype(bf16)
        rights.append(right_both)
        factors.append(left * step)
        transposes.append(
            jnp.concatenate(
                [jnp.transpose(wr * scale), jnp.transpose(kr * scale)], axis=1
            ).astype(bf16)
        )
        left_both = jnp.concatenate([jnp.where(mask, er, 0.0) for mask in own], axis=0)
        grams = mm_nt(left_both.astype(bf16), right_both)
        strict = (row > col) if direction == 0 else (row < col)
        for head in (0, 1):
            rows = slice(head * LEN, (head + 1) * LEN)
            couplings.append(grams[rows, :LEN])
            feeding = jnp.where(strict, grams[rows, LEN:], 0.0).astype(bf16)
            sides.append(jnp.where(own[head], er, mm(feeding, fed_by)))
    couplings = [jnp.where(row > col, couplings[h], couplings[2 + h]) for h in (0, 1)]
    sides = [(sides[h], sides[2 + h]) for h in (0, 1)]
    return couplings, sides, transposes, rights, factors, crossed_values, scale, total


def pairs_terms(inputs):
    row, col = rows_cols()
    setups = [pair_setup(*given, row, col) for given in inputs]
    answers = solve_both(
        [a for setup in setups for a in setup[0]],
        [side for setup in setups for side in setup[1]],
        row,
        col,
    )
    results = []
    for k, setup in enumerate(setups):
        _, _, transposes, rights, factors, crossed_values, scale, total = setup
        maps, solved = [], []
        for direction in (0, 1):
            for head in (0, 1):
                mine = head_mask(head)
                answer = answers[2 * k + head][direction]
                rows = jnp.where(mine, answer * scale, answer).astype(bf16)
                crossed = jnp.where(mine, 0.0, crossed_values).astype(bf16)
                maps.append(state_map(transposes[direction], rows, crossed, total, head))
                solved.append(rows)
        results.append((maps, solved, rights, factors, scale))
    return results


def pair_reads(queries, values, solved, rights, factors, scale):
    row, col = rows_cols()
    own = [head_mask(0), head_mask(1)]
    crossed_values = pltpu.roll(values, HALF, 1)
    crossed = [jnp.where(mask, 0.0, crossed_values).astype(bf16) for mask in own]
    reads = []
    for direction in (0, 1):
        qr = queries * factors[direction]
        left_both = jnp.concatenate([jnp.where(mask, qr, 0.0) for mask in own], axis=0)
        grams = mm_nt(left_both.astype(bf16), rights[direction])
        reach = (row >= col) if direction == 0 else (row <= col)
        both = jnp.concatenate([reach, reach], axis=1)
        for head in (0, 1):
            attend = jnp.where(both, grams[head * LEN : (head + 1) * LEN], 0.0).astype(bf16)
            reads.append(
                mm(attend, jnp.concatenate([solved[2 * direction + head], crossed[head]], axis=0))
                + jnp.where(own[head], qr * scale, 0.0)
            )
    ahead = [jnp.where(own[0], reads[at], reads[at + 1]) for at in (0, 2)]
    local = jnp.where(own[0], reads[1], reads[0]) + jnp.where(own[0], reads[3], reads[2])
    return jnp.concatenate(ahead, axis=1), pltpu.roll(local, HALF, 1)


def context_terms(pairs, lows, bias, backward):
    row, col = rows_cols()
    cross = row ^ col
    own = head_mask(0)
    order = (row - col) * (1 - 2 * backward)
    strict = order > 0
    units = []
    for pair, low in zip(pairs, lows):
        gates = jax.nn.sigmoid(bias + low)
        log_decay = jnp.where(own, -DECAY_TOP * gates, 0.0)
        rate = pltpu.roll(gates, HALF, 1)
        keys = jnp.where(own, pair, 0.0)
        cum = cumulative(log_decay, row, col)
        total = cum[LEN - 1 : LEN]
        half = 0.5 * total
        scale = jnp.exp(half)
        unit = keys * lax.rsqrt(jnp.sum(keys * keys, axis=-1, keepdims=True) + 1.0)
        one, two = cum - log_decay - half, half - cum
        left = jnp.exp(jnp.where(backward == 0, one, two))
        right = jnp.exp(jnp.where(backward == 0, two, one))
        er, wr, kr = -unit * left, unit * rate * right, keys * right
        grams = mm_nt(er.astype(bf16), jnp.concatenate([wr, kr], axis=0).astype(bf16))
        coupling = jnp.where(strict, grams[:, :LEN], 0.0)
        feeding = jnp.where(strict, grams[:, LEN:], 0.0).astype(bf16)
        crossed = jnp.where(own, 0.0, pair).astype(bf16)
        side = jnp.where(own, er, mm(feeding, crossed))
        transposed = jnp.concatenate(
            [jnp.transpose(wr * scale), jnp.transpose(kr * scale)], axis=1
        ).astype(bf16)
        units.append((coupling, side, transposed, crossed, scale, total))
    answers = solve([u[0] for u in units], [u[1] for u in units], cross)
    maps = []
    for (_, _, transposed, crossed, scale, total), answer in zip(units, answers):
        solved = jnp.where(own, answer * scale, answer).astype(bf16)
        maps.append(state_map(transposed, solved, crossed, total, 0))
    return maps


def compose(earlier, later):
    high, low = split(earlier)
    transfer = later[:, :HALF].astype(bf16)
    lane = lax.broadcasted_iota(jnp.int32, (1, LEN), 1)
    return mm(transfer, high) + mm(transfer, low) + jnp.where(lane >= HALF, later, 0.0)


def remote(src, dst, send, recv, sp, tp):
    return pltpu.make_async_remote_copy(
        src_ref=src,
        dst_ref=dst,
        send_sem=send,
        recv_sem=recv,
        device_id=(sp, tp),
        device_id_type=MESH,
    )


def kernel(
    latent,
    context,
    condition,
    context_condition,
    shift_weight,
    scale_weight,
    gate_weight,
    norm_gain,
    decay_down,
    decay_up,
    rate_down,
    rate_up,
    head_bias,
    query_weight,
    key_weight,
    value_weight,
    branch_weight,
    group_gain,
    out_weight,
    out,
    result,
    rows,
    own_rows,
    ctx_rows,
    cond,
    mod_w,
    gain,
    down,
    up,
    bias,
    wq,
    wk,
    wv,
    wb,
    ggain,
    wo,
    part,
    ybuf,
    zpart,
    zbuf,
    mods,
    gpart,
    gbuf,
    gsum,
    gmods,
    normed,
    low,
    kbuf,
    vbuf,
    dbuf,
    rbuf,
    qbuf,
    bbuf,
    ctx_out,
    ctx_in,
    head_rows,
    map_out,
    map_in,
    ctx_maps,
    solved_buf,
    right_buf,
    factor_buf,
    scale_buf,
    ahead,
    local,
    state_out,
    states,
    mixed,
    partial,
    paired,
    summed,
    arrived,
    load,
    y_s,
    y_r,
    z_s,
    z_r,
    t_s,
    t_r,
    l_s,
    l_r,
    f_s,
    c_s,
    c_r,
    m_s,
    m_r,
    s_s,
    s_r,
    o_s,
    o_r,
    g_s,
    g_r,
    gs_s,
    gs_r,
    gt_s,
    gt_r,
):
    sp = lax.axis_index("sp")
    tp = lax.axis_index("tp")
    zz, yy = sp // 4, sp % 4
    xx, core = tp // 2, tp % 2
    sibling = 2 * xx + (1 - core)

    def at_offset(dz, dy):
        return ((zz + dz) % 4) * 4 + (yy + dy) % 4

    width = wq.shape[1]
    model = normed.shape[1]
    blocks = model // width
    own_n = own_rows.shape[0]
    ctx_n = ctx_rows.shape[0]

    scopes = contextlib.ExitStack()

    def phase(name):
        scopes.close()
        scopes.enter_context(jax.named_scope(name))

    phase("greet")
    barrier = pltpu.get_barrier_semaphore()

    for j in (2, 1, 3):
        for to in (zz * 4 + (yy + j) % 4, ((zz + j) % 4) * 4 + yy):
            pl.semaphore_signal(barrier, inc=1, device_id=(to, tp), device_id_type=MESH)
    for j in range(1, N_TP):
        pl.semaphore_signal(
            barrier, inc=1, device_id=(sp, (tp + j) % N_TP), device_id_type=MESH
        )

    def fetch(at, src, dst):
        return pltpu.make_async_copy(src, dst, load.at[at])

    copies = [
        fetch(0, condition, cond.at[0:1]),
        fetch(1, context_condition, cond.at[1:2]),
        fetch(2, shift_weight, mod_w.at[0]),
        fetch(3, scale_weight, mod_w.at[1]),
        fetch(4, gate_weight, mod_w.at[2]),
        fetch(6, context, ctx_rows),
        fetch(7, norm_gain, gain),
        fetch(8, decay_down, down.at[:, 0:LEN]),
        fetch(9, rate_down, down.at[:, LEN : 2 * LEN]),
        fetch(10, decay_up, up.at[0]),
        fetch(11, rate_up, up.at[1]),
        fetch(12, head_bias, bias),
        fetch(13, key_weight, wk),
        fetch(14, value_weight, wv),
        fetch(15, query_weight, wq),
        fetch(16, branch_weight, wb),
        fetch(17, group_gain, ggain),
        fetch(18, out_weight, wo),
    ]
    copies.insert(5, fetch(5, latent, own_rows))
    copies[5].start()
    for copy in copies[:5] + copies[6:]:
        copy.start()

    phase("barrier")
    copies[5].wait()
    pl.semaphore_wait(barrier, 6 + N_TP - 1)
    sends = []

    def start(copy):
        copy.start()
        sends.append(copy)

    for j in (2, 1, 3):
        to = 2 * ((xx + j) % 4) + core
        start(remote(own_rows, rows.at[tp], l_s.at[j], l_r.at[tp], sp, to))
    start(remote(own_rows, rows.at[tp], l_s.at[0], l_r.at[tp], sp, sibling))
    rows[tp] = own_rows[...]

    phase("wait_mod_w")
    for at in (0, 1, 2, 3, 4):
        copies[at].wait()
    phase("shares")
    rows_c = cond[...]
    conditions = (rows_c * jax.nn.sigmoid(rows_c)).astype(bf16)
    conditions = jnp.concatenate([conditions, jnp.zeros((14, rows_c.shape[1]), bf16)], axis=0)
    shares = [mm(conditions, mod_w[at]) for at in range(3)]
    halves = (slice(0, width // 2), slice(width // 2, width))
    part[...] = jnp.concatenate(
        [share[0:2, half] for half in halves for share in shares[:2]], axis=0
    )
    gpart[...] = jnp.concatenate(
        [shares[2][0:1, k * LEN : (k + 1) * LEN] for k in range(width // LEN)]
        + [jnp.zeros((8 - width // LEN, LEN), f32)],
        axis=0,
    )
    ybuf[yy] = part[...]
    gbuf[0, yy] = gpart[...]
    phase("send_y")
    for j in (2, 1, 3):
        to = zz * 4 + (yy + j) % 4
        start(remote(part, ybuf.at[yy], y_s.at[j], y_r.at[yy], to, tp))
    for j in (1, 2, 3):
        to = zz * 4 + (yy + j) % 4
        start(remote(gpart, gbuf.at[0, yy], gs_s.at[0, j], gs_r.at[0, yy], to, tp))
    phase("wait_y")
    for j in (1, 2, 3):
        frm = (yy + j) % 4
        remote(part, ybuf.at[frm], y_s.at[j], y_r.at[frm], sp, tp).wait_recv()
    zpart[...] = ybuf[0] + ybuf[1] + ybuf[2] + ybuf[3]
    zbuf[zz] = zpart[...]
    for j in (2, 1, 3):
        to = ((zz + j) % 4) * 4 + yy
        start(remote(zpart, zbuf.at[zz], z_s.at[j], z_r.at[zz], to, tp))

    phase("ctx_stats")
    copies[6].wait()
    ctx = ctx_rows[...].astype(f32)
    ctx_scale = lax.rsqrt(jnp.mean(ctx * ctx, axis=-1, keepdims=True) + NORM_EPS)

    phase("wait_z")
    for j in (1, 2, 3):
        frm = (zz + j) % 4
        remote(zpart, zbuf.at[frm], z_s.at[j], z_r.at[frm], sp, tp).wait_recv()
    part2 = zbuf[0] + zbuf[1] + zbuf[2] + zbuf[3]
    mods[tp] = part2
    for j in (4, 5, 2, 3, 6, 7, 1):
        to = 2 * ((xx + j // 2) % 4) + (core + j) % 2
        start(remote(mods.at[tp], mods.at[tp], t_s.at[j], t_r.at[tp], sp, to))

    phase("latent_x")
    for j in (1, 3, 2):
        frm = 2 * ((xx + j) % 4) + core
        remote(own_rows, rows.at[frm], l_s.at[j], l_r.at[frm], sp, tp).wait_recv()
        start(remote(rows.at[frm], rows.at[frm], f_s.at[j], l_r.at[frm], sp, sibling))
    phase("latent_core")
    for j in (0, 1, 3, 2):
        frm = 2 * ((xx + j) % 4) + (1 - core)
        remote(own_rows, rows.at[frm], l_s.at[j], l_r.at[frm], sp, tp).wait_recv()
    phase("latent_stats")
    inverses = []
    for i in range(N_TP):
        values = rows[i].astype(f32)
        inverses.append(lax.rsqrt(jnp.mean(values * values, axis=-1, keepdims=True) + NORM_EPS))

    phase("wait_t")
    copies[7].wait()
    for j in range(1, N_TP):
        frm = (tp + j) % N_TP
        remote(part, mods.at[frm], t_s.at[j], t_r.at[frm], sp, tp).wait_recv()

    phase("normalize")
    for j in range(2 * blocks):
        cols = slice(j * width // 2, (j + 1) * width // 2)
        vectors = mods[j // 2, 4 * (j % 2) : 4 * (j % 2) + 4]
        factor = gain[0:1, cols] * (1.0 + vectors[2:3])
        shift = vectors[0:1]
        for i in range(N_TP):
            normed[i * own_n : (i + 1) * own_n, cols] = (
                rows[i, :, cols].astype(f32) * inverses[i] * factor + shift
            ).astype(bf16)
        factor = gain[0:1, cols] * (1.0 + vectors[3:4])
        shift = vectors[1:2]
        normed[LEN : LEN + ctx_n, cols] = (
            ctx_rows[:, cols].astype(f32) * ctx_scale * factor + shift
        ).astype(bf16)

    for j in (1, 2, 3):
        frm = (yy + j) % 4
        remote(gpart, gbuf.at[0, frm], gs_s.at[0, j], gs_r.at[0, frm], sp, tp).wait_recv()
    gsum[0] = gbuf[0, 0] + gbuf[0, 1] + gbuf[0, 2] + gbuf[0, 3]
    gbuf[1, zz] = gsum[0]
    for j in (1, 2, 3):
        to = ((zz + j) % 4) * 4 + yy
        start(remote(gsum.at[0], gbuf.at[1, zz], gs_s.at[1, j], gs_r.at[1, zz], to, tp))

    phase("lows")
    for at in (8, 9, 10, 11, 12):
        copies[at].wait()
    lows = mm(normed[...], down[...])
    low[:, :LEN] = jnp.tanh(lows[:, :LEN]).astype(bf16)
    low[:, LEN:] = lows[:, LEN:].astype(bf16)
    dbuf[...] = mm(low[:, :LEN], up[0]).astype(bf16)
    rbuf[...] = mm(low[:, LEN:], up[1]).astype(bf16)

    def project(weight, to, count):
        def body(i, carry):
            at = pl.ds(pl.multiple_of(i * 256, 256), 256)
            to[:, at] = mm(normed[0:count], weight[:, at]).astype(bf16)
            return carry

        lax.fori_loop(0, width // 256, body, 0)

    phase("proj_kv")
    copies[13].wait()
    project(wk, kbuf, LEN + ctx_n)
    copies[14].wait()
    project(wv, vbuf, LEN + ctx_n)

    phase("ctx_pack")
    lane = lax.broadcasted_iota(jnp.int32, (1, LEN), 1)
    left = lane < HALF
    for p in range(width // LEN):
        cols = slice(p * LEN, (p + 1) * LEN)
        for at, (first, second) in enumerate(((kbuf, vbuf), (dbuf, rbuf))):
            a = first[LEN : LEN + ctx_n, cols].astype(f32)
            b = second[LEN : LEN + ctx_n, cols].astype(f32)
            lanes = slice(at * LEN, (at + 1) * LEN)
            ctx_out[2 * p, :, lanes] = jnp.where(left, a, pltpu.roll(b, HALF, 1)).astype(bf16)
            ctx_out[2 * p + 1, :, lanes] = jnp.where(left, pltpu.roll(a, HALF, 1), b).astype(bf16)
        a = bias[0:1, cols]
        b = bias[1:2, cols]
        head_rows[2 * p : 2 * p + 1] = jnp.where(left, a, pltpu.roll(b, HALF, 1))
        head_rows[2 * p + 1 : 2 * p + 2] = jnp.where(left, pltpu.roll(a, HALF, 1), b)
    my_head = sp % 8
    backward = sp // 8
    ctx_in[sp] = ctx_out[my_head]

    for dz, dy in FAR_FIRST:
        to = at_offset(dz, dy)
        start(
            remote(
                ctx_out.at[to % 8], ctx_in.at[sp], c_s.at[4 * dz + dy], c_r.at[sp], to, tp
            )
        )

    phase("chunks")
    def place(to):
        slot = jnp.where(to == sp, N_SP, sp)
        return slot, jnp.where(to == sp, sibling, tp)

    def chunk():
        inputs, at = [], []
        for k in range(width // LEN):
            p = k
            cols = slice(p * LEN, (p + 1) * LEN)
            gates = jax.nn.sigmoid(bias[0:1, cols] + dbuf[0:LEN, cols].astype(f32))
            rate = jax.nn.sigmoid(bias[1:2, cols] + rbuf[0:LEN, cols].astype(f32))
            inputs.append(
                (
                    kbuf[0:LEN, cols].astype(f32),
                    vbuf[0:LEN, cols].astype(f32),
                    -DECAY_TOP * gates,
                    rate,
                )
            )
            at.append(p)
        found = pairs_terms(inputs)
        for p, (maps, solved, rights, factors, scale) in zip(at, found):
            for direction in (0, 1):
                for head in (0, 1):
                    map_out[direction * 8 + 2 * p + head] = maps[2 * direction + head].astype(bf16)
        for dz, dy in FAR_FIRST:
            to = at_offset(dz, dy)
            start(remote(map_out.at[to], map_in.at[sp], m_s.at[to], m_r.at[sp], to, tp))
        for p, (maps, solved, rights, factors, scale) in zip(at, found):
            for direction in (0, 1):
                for head in (0, 1):
                    solved_buf[p, 2 * direction + head] = solved[2 * direction + head]
                right_buf[p, direction] = rights[direction]
                factor_buf[p, direction] = factors[direction]
            scale_buf[p] = scale

    chunk()
    map_in[sp] = map_out[sp]

    for j in (1, 2, 3):
        frm = (zz + j) % 4
        remote(gpart, gbuf.at[1, frm], gs_s.at[1, j], gs_r.at[1, frm], sp, tp).wait_recv()
    gmods[tp] = gbuf[1, 0] + gbuf[1, 1] + gbuf[1, 2] + gbuf[1, 3]
    for j in range(1, N_TP):
        to = (tp + j) % N_TP
        start(remote(gmods.at[tp], gmods.at[tp], gt_s.at[j], gt_r.at[tp], sp, to))

    phase("wait_ctx")
    for j in range(1, N_SP):
        frm = (sp + j) % N_SP
        remote(ctx_out.at[0], ctx_in.at[frm], c_s.at[j], c_r.at[frm], sp, tp).wait_recv()
    phase("ctx_chunks")
    my_bias = head_rows[pl.ds(my_head, 1)]
    per = LEN // ctx_n
    pairs, lows_in = [], []
    for c in range(N_SP // per):
        pairs.append(ctx_in[c * per : (c + 1) * per, :, 0:LEN].astype(f32).reshape(LEN, LEN))
        lows_in.append(ctx_in[c * per : (c + 1) * per, :, LEN:].astype(f32).reshape(LEN, LEN))
    for c, found in enumerate(context_terms(pairs, lows_in, my_bias, backward)):
        ctx_maps[c] = found
    phase("proj_b")
    copies[16].wait()
    project(wb, bbuf, LEN)
    phase("wait_maps")
    for copy in sends:
        copy.wait_send()
    drained = len(sends)
    for j in range(1, N_SP):
        frm = (sp + j) % N_SP
        remote(map_out.at[0], map_in.at[frm], m_s.at[0], m_r.at[frm], sp, tp).wait_recv()
    phase("walk")
    count = N_SP // per
    forward = backward == 0
    order = [jnp.where(forward, i, N_SP - 1 - i) for i in range(N_SP)]
    steps = [map_in[order[i]].astype(f32) for i in range(N_SP - 1)]
    state = ctx_maps[jnp.where(forward, 0, count - 1)]
    for c in range(1, count):
        state = compose(state, ctx_maps[jnp.where(forward, c, count - 1 - c)])
    two = [compose(steps[2 * i], steps[2 * i + 1]) for i in range(7)]
    four = [compose(two[2 * i], two[2 * i + 1]) for i in range(3)]
    eight = compose(four[0], four[1])
    odd = my_head % 2
    left = lax.broadcasted_iota(jnp.int32, (1, LEN), 1) < HALF

    def show(i, state):
        to = order[i]
        state_out[to] = jnp.where(
            left, pltpu.roll(state[: HALF // 2], HALF, 1), state[HALF // 2 :]
        ).astype(bf16)

    def launch(to):
        slot, over = place(to)
        remote(state_out.at[to], states.at[slot], s_s.at[to], s_r.at[slot], to, over).start()

    held = {0: state}
    show(0, state)
    held[8] = compose(state, eight)
    held[4] = compose(state, four[0])
    show(8, held[8])
    show(4, held[4])
    for i in (0, 8, 4):
        launch(order[i])
    held[12] = compose(held[8], four[2])
    held[2] = compose(state, two[0])
    held[6] = compose(held[4], two[2])
    held[10] = compose(held[8], two[4])
    held[14] = compose(held[12], two[6])
    for i in (2, 6, 10, 12, 14):
        show(i, held[i])
    for i in (2, 6, 10, 12, 14):
        launch(order[i])
    for i in range(1, N_SP, 2):
        show(i, compose(held[i - 1], steps[i - 1]))
    even = (yy % 2 == 0) == (backward == 1)
    for one, other in zip(EVEN_FIRST, ODD_FIRST):
        launch(jnp.where(even, at_offset(*one), at_offset(*other)))
    states[sp] = state_out[sp]

    phase("proj_qb")
    copies[15].wait()
    project(wq, qbuf, LEN)
    phase("read_terms")

    def read_terms(p, carry):
        cols = pl.ds(pl.multiple_of(p * LEN, LEN), LEN)
        coming, here = pair_reads(
            qbuf[:, cols].astype(f32),
            vbuf[0:LEN, cols].astype(f32),
            [solved_buf[p, i] for i in range(4)],
            [right_buf[p, i] for i in range(2)],
            [factor_buf[p, i] for i in range(2)],
            scale_buf[p],
        )
        ahead[p] = coming.astype(bf16)
        local[p] = here
        return carry

    lax.fori_loop(0, width // LEN, read_terms, 0)

    phase("wait_states")
    for j in range(1, N_SP + 1):
        frm = (sp + j) % N_SP if j < N_SP else N_SP
        remote(state_out.at[0], states.at[frm], s_s.at[0], s_r.at[frm], sp, tp).wait_recv()

    phase("reads")
    for j in range(1, N_TP):
        frm = (tp + j) % N_TP
        remote(gpart, gmods.at[frm], gt_s.at[j], gt_r.at[frm], sp, tp).wait_recv()
    copies[17].wait()
    other = lane >= HALF
    for p in range(width // LEN):
        cols = slice(p * LEN, (p + 1) * LEN)
        blocks_in = []
        for at in (2 * p, 8 + 2 * p):
            first, second = states[at].astype(f32), states[at + 1].astype(f32)
            blocks_in += [
                jnp.where(left, first, 0.0),
                jnp.where(left, pltpu.roll(first, HALF, 1), 0.0),
                jnp.where(left, 0.0, pltpu.roll(second, HALF, 1)),
                jnp.where(left, 0.0, second),
            ]
        both = jnp.concatenate(blocks_in, axis=0).astype(bf16)
        reads = mm(ahead[p], both) + local[p]

        def head_mean(x):
            sums = [
                jnp.sum(jnp.where(mask, x, 0.0), axis=-1, keepdims=True) for mask in (left, other)
            ]
            return jnp.where(left, sums[0], sums[1]) * (1.0 / HALF)

        centred = reads - head_mean(reads)
        normal = centred * lax.rsqrt(head_mean(centred * centred) + GROUP_EPS)
        gate = bbuf[:, cols].astype(f32)
        mixed[:, cols] = (
            normal * ggain[0:1, cols] * (gate * jax.nn.sigmoid(gate))
        ).astype(bf16)

    phase("out_proj")
    copies[18].wait()
    n_chunk = arrived.shape[0]
    piece = model // n_chunk

    def chip_sum(c, x):
        return partial[c, core, x].astype(f32) + paired[c, x].astype(f32)

    def send_x(c, j):
        x = (xx + j) % 4
        start(
            remote(
                summed.at[c, j - 1], arrived.at[c, j - 1], g_s.at[c, j - 1], g_r.at[c, j - 1], sp,
                2 * x + core,
            )
        )

    def pass_on(c):
        remote(partial.at[c, 0], paired.at[c], o_s.at[c], o_r.at[c], sp, tp).wait_recv()
        for j in (2, 1, 3):
            summed[c, j - 1] = chip_sum(c, (xx + j) % 4).astype(bf16)
        send_x(c, 2)
        if c % 2 == 1:
            for at in (c - 1, c):
                send_x(at, 1)
                send_x(at, 3)

    for c in range(n_chunk):
        cols = slice(c * piece, (c + 1) * piece)
        product = mm(mixed[...], wo[:, cols]).astype(bf16)
        for x in range(4):
            for k in range(2):
                lo = (2 * x + k) * own_n
                partial[c, k, x] = product[lo : lo + own_n]
        start(
            remote(
                partial.at[c, 1 - core], paired.at[c], o_s.at[c], o_r.at[c], sp, sibling
            )
        )
        if c >= lag:
            pass_on(c - lag)
    phase("wait_core")
    for c in range(n_chunk - lag, n_chunk):
        pass_on(c)
    phase("wait_x")
    pieces = []
    for c in range(n_chunk):
        for k in (0, 2, 1):
            remote(
                summed.at[c, 0], arrived.at[c, k], g_s.at[c, k], g_r.at[c, k], sp, tp
            ).wait_recv()
        total = chip_sum(c, xx)
        for k in range(3):
            total = total + arrived[c, k].astype(f32)
        pieces.append(total.astype(bf16).astype(f32))
    phase("final")
    square = sum(jnp.sum(p * p, axis=-1, keepdims=True) for p in pieces)
    inverse = lax.rsqrt(square * (1.0 / model) + NORM_EPS)
    for c in range(n_chunk):
        for k in range(piece // LEN):
            lo = c * piece + k * LEN
            cols = slice(lo, lo + LEN)
            lane_block = lo // LEN
            per_tp = width // LEN
            gate = gmods[lane_block // per_tp, lane_block % per_tp : lane_block % per_tp + 1]
            value = pieces[c][:, k * LEN : (k + 1) * LEN]
            result[:, cols] = (own_rows[:, cols].astype(f32) + gate * (value * inverse)).astype(bf16)

    phase("drain")
    put = pltpu.make_async_copy(result, out, load.at[0])
    put.start()
    for copy in sends[drained:]:
        copy.wait_send()

    for j in range(N_SP):
        remote(state_out.at[0], states.at[0], s_s.at[j], s_r.at[0], sp, tp).wait_send()
    put.wait()
    scopes.close()


def on_device(
    latent,
    context,
    condition,
    context_condition,
    shift_weight,
    scale_weight,
    gate_weight,
    norm_gain,
    decay_down,
    decay_up,
    rate_down,
    rate_up,
    head_bias,
    query_weight,
    key_weight,
    value_weight,
    branch_weight,
    group_gain,
    out_weight,
):
    own_n, model = latent.shape
    ctx_n = context.shape[0]
    width = query_weight.shape[1]
    held = condition.shape[0]
    args = (
        latent,
        context,
        condition.reshape(1, -1),
        context_condition.reshape(1, -1),
        shift_weight,
        scale_weight,
        gate_weight,
        norm_gain.reshape(1, -1),
        decay_down,
        decay_up,
        rate_down,
        rate_up,
        head_bias,
        query_weight,
        key_weight,
        value_weight,
        branch_weight,
        group_gain.reshape(1, -1),
        out_weight,
    )
    n_chunk = 8
    piece = model // n_chunk
    V = pltpu.VMEM
    dma = pltpu.SemaphoreType.DMA
    scratch = [
        V((own_n, model), bf16),
        V((N_TP, own_n, model), bf16),
        V((own_n, model), bf16),
        V((ctx_n, model), bf16),
        V((2, held), f32),
        V((3, held, width), bf16),
        V((1, model), f32),
        V((model, 2 * LEN), bf16),
        V((2, LEN, width), bf16),
        V((2, width), f32),
        V((model, width), bf16),
        V((model, width), bf16),
        V((model, width), bf16),
        V((model, width), bf16),
        V((1, width), f32),
        V((width, model), bf16),
        V((8, width // 2), f32),
        V((4, 8, width // 2), f32),
        V((8, width // 2), f32),
        V((4, 8, width // 2), f32),
        V((N_TP, 8, width // 2), f32),
        V((8, LEN), f32),
        V((2, 4, 8, LEN), f32),
        V((1, 8, LEN), f32),
        V((N_TP, 8, LEN), f32),
        V((LEN + ctx_n, model), bf16),
        V((LEN + ctx_n, 2 * LEN), bf16),
        V((LEN + ctx_n, width), bf16),
        V((LEN + ctx_n, width), bf16),
        V((LEN + ctx_n, width), bf16),
        V((LEN + ctx_n, width), bf16),
        V((LEN, width), bf16),
        V((LEN, width), bf16),
        V((8, ctx_n, 2 * LEN), bf16),
        V((N_SP, ctx_n, 2 * LEN), bf16),
        V((8, LEN), f32),
        V((N_SP, HALF, LEN), bf16),
        V((N_SP + 1, HALF, LEN), bf16),
        V((4, HALF, LEN), f32),
        V((width // LEN, 4, LEN, LEN), bf16),
        V((width // LEN, 2, 2 * LEN, LEN), bf16),
        V((width // LEN, 2, LEN, LEN), f32),
        V((width // LEN, 1, LEN), f32),
        V((width // LEN, LEN, 2 * LEN), bf16),
        V((width // LEN, LEN, LEN), f32),
        V((N_SP, HALF // 2, LEN), bf16),
        V((N_SP + 1, HALF // 2, LEN), bf16),
        V((LEN, width), bf16),
        V((n_chunk, 2, 4, own_n, piece), bf16),
        V((n_chunk, 4, own_n, piece), bf16),
        V((n_chunk, 3, own_n, piece), bf16),
        V((n_chunk, 3, own_n, piece), bf16),
        dma((19,)),
        dma((4,)),
        dma((4,)),
        dma((4,)),
        dma((4,)),
        dma((N_TP,)),
        dma((N_TP,)),
        dma((4,)),
        dma((N_TP,)),
        dma((4,)),
        dma((N_SP,)),
        dma((N_SP,)),
        dma((N_SP,)),
        dma((N_SP + 1,)),
        dma((N_SP,)),
        dma((N_SP + 1,)),
        dma((n_chunk,)),
        dma((n_chunk,)),
        dma((n_chunk, 3)),
        dma((n_chunk, 3)),
        dma((2, 4)),
        dma((2, 4)),
        dma((N_TP,)),
        dma((N_TP,)),
    ]
    return pl.pallas_call(
        kernel,
        out_shape=jax.ShapeDtypeStruct((own_n, model), bf16),
        in_specs=[pl.BlockSpec(memory_space=pltpu.HBM)] * len(args),
        out_specs=pl.BlockSpec(memory_space=pl.ANY),
        scratch_shapes=scratch,
        compiler_params=pltpu.CompilerParams(
            collective_id=0, has_side_effects=True, vmem_limit_bytes=44 * 1024 * 1024
        ),
    )(*(pltpu.with_memory_space_constraint(a, pltpu.HBM) for a in args))


def solution(mesh):
    placed = (
        P(("sp", "tp"), None),
        P("sp", None),
        P("sp"),
        P("sp"),
        P("sp", "tp"),
        P("sp", "tp"),
        P("sp", "tp"),
        P(),
        P(),
        P(None, "tp"),
        P(),
        P(None, "tp"),
        P(None, "tp"),
        P(None, "tp"),
        P(None, "tp"),
        P(None, "tp"),
        P(None, "tp"),
        P("tp"),
        P("tp", None),
    )
    return jax.shard_map(
        on_device, mesh=mesh, in_specs=placed, out_specs=P(("sp", "tp"), None), check_vma=False
    )
```

```python
import contextlib
import math

import jax
import jax.numpy as jnp
from jax import lax
from jax.experimental import pallas as pl
from jax.experimental.pallas import tpu as pltpu
from jax.sharding import PartitionSpec as P

HEAD_DIM = 64
NORM_EPS = 1e-06
GROUP_EPS = 0.00064
DECAY_TOP = math.exp(-0.5)
MESH = pl.DeviceIdType.MESH
bf16 = jnp.bfloat16
f32 = jnp.float32
LEN = 128
lag = 5
N_SP = 16
N_TP = 8
HALF = 64
FAR_FIRST = (
    (2, 2), (2, 1), (2, 3), (1, 2), (3, 2), (1, 1), (3, 3), (1, 3), (3, 1),
    (2, 0), (0, 2), (1, 0), (3, 0), (0, 1), (0, 3),
)


def mm(a, b):
    return jnp.dot(a, b, preferred_element_type=f32)


def mm_nt(a, b):
    return lax.dot_general(a, b, (((1,), (1,)), ((), ())), preferred_element_type=f32)


def split(a):
    high = a.astype(bf16)
    return high, (a - high.astype(f32)).astype(bf16)


def rows_cols():
    row = lax.broadcasted_iota(jnp.int32, (LEN, LEN), 0)
    col = lax.broadcasted_iota(jnp.int32, (LEN, LEN), 1)
    return row, col


def cumulative(log_decay, row, col):
    lower = jnp.where(row >= col, 1.0, 0.0).astype(bf16)
    high, low = split(log_decay)
    return mm(lower, high) + mm(lower, low)


def solve(couplings, sides, cross):
    row, col = rows_cols()
    eye = jnp.where(row == col, 1.0, 0.0)
    inverse = [eye + jnp.where(cross == 1, a, 0.0) for a in couplings]
    size = 2
    while size < LEN // 2:
        level = (cross >= size) & (cross < 2 * size)
        low = [d.astype(bf16) for d in inverse]
        part = [mm(jnp.where(level, a, 0.0).astype(bf16), d) for a, d in zip(couplings, low)]
        inverse = [d + mm(e, p.astype(bf16)) for d, e, p in zip(inverse, low, part)]
        size *= 2
    level = (cross >= size) & (cross < 2 * size)
    low = [d.astype(bf16) for d in inverse]
    first = [mm(d, s.astype(bf16)) for d, s in zip(low, sides)]
    part = [
        mm(jnp.where(level, a, 0.0).astype(bf16), y.astype(bf16)) for a, y in zip(couplings, first)
    ]
    return [y + mm(d, p.astype(bf16)) for y, d, p in zip(first, low, part)]


def solve_both(couplings, sides, row, col):
    cross = row ^ col
    lower, upper = row >= col, row <= col
    eye = jnp.where(row == col, 1.0, 0.0)
    held = [eye + jnp.where(cross == 1, a, 0.0) for a in couplings]
    size = 2
    while size < LEN // 2:
        late = (row & size) != 0
        level = (cross >= size) & (cross < 2 * size)
        inner = (late & upper) | (~late & lower)
        outer = (late & lower) | (~late & upper)
        part = [
            mm(jnp.where(level, a, 0.0).astype(bf16), jnp.where(inner, h, 0.0).astype(bf16))
            for a, h in zip(couplings, held)
        ]
        held = [
            h + mm(jnp.where(outer, h, 0.0).astype(bf16), p.astype(bf16))
            for h, p in zip(held, part)
        ]
        size *= 2
    late = (row & size) != 0
    level = (cross >= size) & (cross < 2 * size)
    outer = (late & lower) | (~late & upper)
    first = [
        (
            mm(jnp.where(lower, h, 0.0).astype(bf16), f.astype(bf16)),
            mm(jnp.where(upper, h, 0.0).astype(bf16), b.astype(bf16)),
        )
        for h, (f, b) in zip(held, sides)
    ]
    part = [
        mm(jnp.where(level, a, 0.0).astype(bf16), jnp.where(late, b, f).astype(bf16))
        for a, (f, b) in zip(couplings, first)
    ]
    last = [
        mm(jnp.where(outer, h, 0.0).astype(bf16), p.astype(bf16)) for h, p in zip(held, part)
    ]
    return [
        (f + jnp.where(late, u, 0.0), b + jnp.where(late, 0.0, u))
        for (f, b), u in zip(first, last)
    ]


def head_mask(head):
    lane = lax.broadcasted_iota(jnp.int32, (1, LEN), 1)
    return (lane >= HALF) if head else (lane < HALF)


def pair_unit(keys):
    own = head_mask(0)
    square = keys * keys
    sums = [
        jnp.sum(jnp.where(mask, square, 0.0), axis=-1, keepdims=True)
        for mask in (own, head_mask(1))
    ]
    return keys * lax.rsqrt(jnp.where(own, sums[0], sums[1]) + 1.0)


def state_map(transposed, solved, crossed, total, head):
    lo = head * HALF
    out = mm(
        transposed[lo : lo + HALF], jnp.concatenate([solved, crossed], axis=0)
    )
    row = lax.broadcasted_iota(jnp.int32, (HALF, LEN), 0)
    lane = lax.broadcasted_iota(jnp.int32, (HALF, LEN), 1)
    out = out + jnp.where(lane == row + lo, jnp.exp(total), 0.0)
    return pltpu.roll(out, HALF, 1) if head else out


def pairs_terms(inputs, keep):
    row, col = rows_cols()
    own = [head_mask(0), head_mask(1)]
    cums = [cumulative(log_decay, row, col) for _, _, log_decay, _ in inputs]
    stages = []
    for k, ((keys, values, log_decay, rate), cum) in enumerate(zip(inputs, cums)):
        total = cum[LEN - 1 : LEN]
        half = 0.5 * total
        scale = jnp.exp(half)
        unit = pair_unit(keys)
        erase = -unit
        write = unit * rate
        before = jnp.exp(cum - log_decay - half)
        after = jnp.exp(half - cum)
        step = jnp.exp(log_decay)
        erases, grams, transposes, rights, factors = [], [], [], [], []
        for direction in (0, 1):
            left, right = (before, after) if direction == 0 else (after, before)
            er = erase * left
            wr, kr = write * right, keys * right
            right_both = jnp.concatenate([wr, kr], axis=0).astype(bf16)
            left_both = jnp.concatenate([jnp.where(mask, er, 0.0) for mask in own], axis=0)
            grams.append(mm_nt(left_both.astype(bf16), right_both))
            erases.append(er)
            rights.append(right_both)
            factors.append(left * step)
            transposes.append(
                jnp.concatenate(
                    [jnp.transpose(wr * scale), jnp.transpose(kr * scale)], axis=1
                ).astype(bf16)
            )
        keep(k, rights, factors, scale)
        stages.append((erases, grams, transposes, pltpu.roll(values, HALF, 1), scale, total))
    couplings, sides = [], []
    for erases, grams, _, crossed_values, _, _ in stages:
        fed_by = crossed_values.astype(bf16)
        for head in (0, 1):
            rows = slice(head * LEN, (head + 1) * LEN)
            couplings.append(jnp.where(row > col, grams[0][rows, :LEN], grams[1][rows, :LEN]))
            pair = []
            for direction in (0, 1):
                strict = (row > col) if direction == 0 else (row < col)
                feeding = jnp.where(strict, grams[direction][rows, LEN:], 0.0).astype(bf16)
                pair.append(jnp.where(own[head], erases[direction], mm(feeding, fed_by)))
            sides.append(tuple(pair))
    answers = solve_both(couplings, sides, row, col)
    results = []
    for k, (_, _, transposes, crossed_values, scale, total) in enumerate(stages):
        maps, solved = [], []
        for direction in (0, 1):
            for head in (0, 1):
                mine = own[head]
                answer = answers[2 * k + head][direction]
                rows = jnp.where(mine, answer * scale, answer).astype(bf16)
                crossed = jnp.where(mine, 0.0, crossed_values).astype(bf16)
                maps.append(state_map(transposes[direction], rows, crossed, total, head))
                solved.append(rows)
        results.append((maps, solved))
    return results


def pair_reads(queries, values, solved, rights, factors, scale):
    row, col = rows_cols()
    own = [head_mask(0), head_mask(1)]
    crossed_values = pltpu.roll(values, HALF, 1)
    crossed = [jnp.where(mask, 0.0, crossed_values).astype(bf16) for mask in own]
    reads = []
    for direction in (0, 1):
        qr = queries * factors[direction]
        left_both = jnp.concatenate([jnp.where(mask, qr, 0.0) for mask in own], axis=0)
        grams = mm_nt(left_both.astype(bf16), rights[direction])
        reach = (row >= col) if direction == 0 else (row <= col)
        both = jnp.concatenate([reach, reach], axis=1)
        for head in (0, 1):
            attend = jnp.where(both, grams[head * LEN : (head + 1) * LEN], 0.0).astype(bf16)
            reads.append(
                mm(attend, jnp.concatenate([solved[2 * direction + head], crossed[head]], axis=0))
                + jnp.where(own[head], qr * scale, 0.0)
            )
    ahead = [jnp.where(own[0], reads[at], reads[at + 1]) for at in (0, 2)]
    local = jnp.where(own[0], reads[1], reads[0]) + jnp.where(own[0], reads[3], reads[2])
    return jnp.concatenate(ahead, axis=1), pltpu.roll(local, HALF, 1)


def context_terms(pairs, lows, bias, backward):
    row, col = rows_cols()
    cross = row ^ col
    own = head_mask(0)
    order = (row - col) * (1 - 2 * backward)
    strict = order > 0
    gated = []
    for low in lows:
        gates = jax.nn.sigmoid(bias + low)
        log_decay = jnp.where(own, -DECAY_TOP * gates, 0.0)
        gated.append((log_decay, pltpu.roll(gates, HALF, 1), cumulative(log_decay, row, col)))
    stages = []
    for pair, (log_decay, rate, cum) in zip(pairs, gated):
        keys = jnp.where(own, pair, 0.0)
        total = cum[LEN - 1 : LEN]
        half = 0.5 * total
        scale = jnp.exp(half)
        unit = keys * lax.rsqrt(jnp.sum(keys * keys, axis=-1, keepdims=True) + 1.0)
        one, two = cum - log_decay - half, half - cum
        left = jnp.exp(jnp.where(backward == 0, one, two))
        right = jnp.exp(jnp.where(backward == 0, two, one))
        er, wr, kr = -unit * left, unit * rate * right, keys * right
        grams = mm_nt(er.astype(bf16), jnp.concatenate([wr, kr], axis=0).astype(bf16))
        transposed = jnp.concatenate(
            [jnp.transpose(wr * scale), jnp.transpose(kr * scale)], axis=1
        ).astype(bf16)
        crossed = jnp.where(own, 0.0, pair).astype(bf16)
        stages.append((grams, er, transposed, crossed, scale, total))
    units = []
    for grams, er, transposed, crossed, scale, total in stages:
        coupling = jnp.where(strict, grams[:, :LEN], 0.0)
        feeding = jnp.where(strict, grams[:, LEN:], 0.0).astype(bf16)
        side = jnp.where(own, er, mm(feeding, crossed))
        units.append((coupling, side, transposed, crossed, scale, total))
    answers = solve([u[0] for u in units], [u[1] for u in units], cross)
    maps = []
    for (_, _, transposed, crossed, scale, total), answer in zip(units, answers):
        solved = jnp.where(own, answer * scale, answer).astype(bf16)
        maps.append(state_map(transposed, solved, crossed, total, 0))
    return maps


def compose(earlier, later):
    high, low = split(earlier)
    transfer = later[:, :HALF].astype(bf16)
    lane = lax.broadcasted_iota(jnp.int32, (1, LEN), 1)
    return mm(transfer, high) + mm(transfer, low) + jnp.where(lane >= HALF, later, 0.0)


def remote(src, dst, send, recv, sp, tp):
    return pltpu.make_async_remote_copy(
        src_ref=src,
        dst_ref=dst,
        send_sem=send,
        recv_sem=recv,
        device_id=(sp, tp),
        device_id_type=MESH,
    )


def kernel(
    latent,
    context,
    condition,
    context_condition,
    shift_weight,
    scale_weight,
    gate_weight,
    norm_gain,
    decay_down,
    decay_up,
    rate_down,
    rate_up,
    head_bias,
    query_weight,
    key_weight,
    value_weight,
    branch_weight,
    group_gain,
    out_weight,
    out,
    result,
    rows,
    own_rows,
    ctx_rows,
    cond,
    mod_w,
    gain,
    down,
    up,
    bias,
    wq,
    wk,
    wv,
    wb,
    ggain,
    wo,
    part,
    ybuf,
    zpart,
    zbuf,
    mods,
    gpart,
    gbuf,
    gsum,
    gmods,
    normed,
    low,
    kbuf,
    vbuf,
    dbuf,
    rbuf,
    qbuf,
    bbuf,
    ctx_out,
    ctx_in,
    head_rows,
    map_out,
    map_in,
    ctx_maps,
    ctx_state,
    solved_buf,
    right_buf,
    factor_buf,
    scale_buf,
    ahead,
    local,
    state_out,
    states,
    mixed,
    partial,
    paired,
    summed,
    arrived,
    load,
    y_s,
    y_r,
    z_s,
    z_r,
    t_s,
    t_r,
    l_s,
    l_r,
    f_s,
    c_s,
    c_r,
    m_s,
    m_r,
    s_s,
    s_r,
    o_s,
    o_r,
    g_s,
    g_r,
    gs_s,
    gs_r,
    gt_s,
    gt_r,
):
    sp = lax.axis_index("sp")
    tp = lax.axis_index("tp")
    zz, yy = sp // 4, sp % 4
    xx, core = tp // 2, tp % 2
    sibling = 2 * xx + (1 - core)

    def at_offset(dz, dy):
        return ((zz + dz) % 4) * 4 + (yy + dy) % 4

    width = wq.shape[1]
    model = normed.shape[1]
    blocks = model // width
    own_n = own_rows.shape[0]
    ctx_n = ctx_rows.shape[0]

    scopes = contextlib.ExitStack()

    def phase(name):
        scopes.close()
        scopes.enter_context(jax.named_scope(name))

    phase("greet")
    barrier = pltpu.get_barrier_semaphore()

    for j in (2, 1, 3):
        for to in (zz * 4 + (yy + j) % 4, ((zz + j) % 4) * 4 + yy):
            pl.semaphore_signal(barrier, inc=1, device_id=(to, tp), device_id_type=MESH)
    for j in range(1, N_TP):
        pl.semaphore_signal(
            barrier, inc=1, device_id=(sp, (tp + j) % N_TP), device_id_type=MESH
        )

    def fetch(at, src, dst):
        return pltpu.make_async_copy(src, dst, load.at[at])

    copies = [
        fetch(0, condition, cond.at[0:1]),
        fetch(1, context_condition, cond.at[1:2]),
        fetch(2, shift_weight, mod_w.at[0]),
        fetch(3, scale_weight, mod_w.at[1]),
        fetch(4, gate_weight, mod_w.at[2]),
        fetch(6, context, ctx_rows),
        fetch(7, norm_gain, gain),
        fetch(8, decay_down, down.at[:, 0:LEN]),
        fetch(9, rate_down, down.at[:, LEN : 2 * LEN]),
        fetch(10, decay_up, up.at[0]),
        fetch(11, rate_up, up.at[1]),
        fetch(12, head_bias, bias),
        fetch(13, key_weight, wk),
        fetch(14, value_weight, wv),
        fetch(15, query_weight, wq),
        fetch(16, branch_weight, wb),
        fetch(17, group_gain, ggain),
        fetch(18, out_weight, wo),
    ]
    copies.insert(5, fetch(5, latent, own_rows))
    copies[5].start()
    for copy in copies[:5] + copies[6:]:
        copy.start()

    phase("barrier")
    copies[5].wait()
    pl.semaphore_wait(barrier, 6 + N_TP - 1)
    sends = []

    def start(copy):
        copy.start()
        sends.append(copy)

    for j in (2, 1, 3):
        to = 2 * ((xx + j) % 4) + core
        start(remote(own_rows, rows.at[tp], l_s.at[j], l_r.at[tp], sp, to))
    start(remote(own_rows, rows.at[tp], l_s.at[0], l_r.at[tp], sp, sibling))
    rows[tp] = own_rows[...]

    phase("wait_mod_w")
    for at in (0, 1, 2, 3, 4):
        copies[at].wait()
    phase("shares")
    rows_c = cond[...]
    conditions = (rows_c * jax.nn.sigmoid(rows_c)).astype(bf16)
    conditions = jnp.concatenate([conditions, jnp.zeros((14, rows_c.shape[1]), bf16)], axis=0)
    shares = [mm(conditions, mod_w[at]) for at in range(3)]
    halves = (slice(0, width // 2), slice(width // 2, width))
    part[...] = jnp.concatenate(
        [share[0:2, half] for half in halves for share in shares[:2]], axis=0
    )
    gpart[...] = jnp.concatenate(
        [shares[2][0:1, k * LEN : (k + 1) * LEN] for k in range(width // LEN)]
        + [jnp.zeros((8 - width // LEN, LEN), f32)],
        axis=0,
    )
    ybuf[yy] = part[...]
    gbuf[0, yy] = gpart[...]
    phase("send_y")
    for j in (2, 1, 3):
        to = zz * 4 + (yy + j) % 4
        start(remote(part, ybuf.at[yy], y_s.at[j], y_r.at[yy], to, tp))
    for j in (1, 2, 3):
        to = zz * 4 + (yy + j) % 4
        start(remote(gpart, gbuf.at[0, yy], gs_s.at[0, j], gs_r.at[0, yy], to, tp))
    phase("wait_y")
    for j in (1, 2, 3):
        frm = (yy + j) % 4
        remote(part, ybuf.at[frm], y_s.at[j], y_r.at[frm], sp, tp).wait_recv()
    zpart[...] = ybuf[0] + ybuf[1] + ybuf[2] + ybuf[3]
    zbuf[zz] = zpart[...]
    for j in (2, 1, 3):
        to = ((zz + j) % 4) * 4 + yy
        start(remote(zpart, zbuf.at[zz], z_s.at[j], z_r.at[zz], to, tp))

    phase("ctx_stats")
    copies[6].wait()
    ctx = ctx_rows[...].astype(f32)
    ctx_scale = lax.rsqrt(jnp.mean(ctx * ctx, axis=-1, keepdims=True) + NORM_EPS)

    phase("wait_z")
    for j in (1, 2, 3):
        frm = (zz + j) % 4
        remote(zpart, zbuf.at[frm], z_s.at[j], z_r.at[frm], sp, tp).wait_recv()
    part2 = zbuf[0] + zbuf[1] + zbuf[2] + zbuf[3]
    mods[tp] = part2
    for j in (4, 5, 2, 3, 6, 7, 1):
        to = 2 * ((xx + j // 2) % 4) + (core + j) % 2
        start(remote(mods.at[tp], mods.at[tp], t_s.at[j], t_r.at[tp], sp, to))

    phase("latent_x")
    for j in (1, 3, 2):
        frm = 2 * ((xx + j) % 4) + core
        remote(own_rows, rows.at[frm], l_s.at[j], l_r.at[frm], sp, tp).wait_recv()
        start(remote(rows.at[frm], rows.at[frm], f_s.at[j], l_r.at[frm], sp, sibling))
    phase("latent_core")
    for j in (0, 1, 3, 2):
        frm = 2 * ((xx + j) % 4) + (1 - core)
        remote(own_rows, rows.at[frm], l_s.at[j], l_r.at[frm], sp, tp).wait_recv()
    phase("latent_stats")
    inverses = []
    for i in range(N_TP):
        values = rows[i].astype(f32)
        inverses.append(lax.rsqrt(jnp.mean(values * values, axis=-1, keepdims=True) + NORM_EPS))

    phase("wait_t")
    copies[7].wait()
    for j in range(1, N_TP):
        frm = (tp + j) % N_TP
        remote(part, mods.at[frm], t_s.at[j], t_r.at[frm], sp, tp).wait_recv()

    phase("normalize")
    for j in range(2 * blocks):
        cols = slice(j * width // 2, (j + 1) * width // 2)
        vectors = mods[j // 2, 4 * (j % 2) : 4 * (j % 2) + 4]
        factor = gain[0:1, cols] * (1.0 + vectors[2:3])
        shift = vectors[0:1]
        for i in range(N_TP):
            normed[i * own_n : (i + 1) * own_n, cols] = (
                rows[i, :, cols].astype(f32) * inverses[i] * factor + shift
            ).astype(bf16)
        factor = gain[0:1, cols] * (1.0 + vectors[3:4])
        shift = vectors[1:2]
        normed[LEN : LEN + ctx_n, cols] = (
            ctx_rows[:, cols].astype(f32) * ctx_scale * factor + shift
        ).astype(bf16)

    for j in (1, 2, 3):
        frm = (yy + j) % 4
        remote(gpart, gbuf.at[0, frm], gs_s.at[0, j], gs_r.at[0, frm], sp, tp).wait_recv()
    gsum[0] = gbuf[0, 0] + gbuf[0, 1] + gbuf[0, 2] + gbuf[0, 3]
    gbuf[1, zz] = gsum[0]
    for j in (1, 2, 3):
        to = ((zz + j) % 4) * 4 + yy
        start(remote(gsum.at[0], gbuf.at[1, zz], gs_s.at[1, j], gs_r.at[1, zz], to, tp))

    phase("lows")
    for at in (8, 9, 10, 11, 12):
        copies[at].wait()
    lows = mm(normed[...], down[...])
    low[:, :LEN] = jnp.tanh(lows[:, :LEN]).astype(bf16)
    low[:, LEN:] = lows[:, LEN:].astype(bf16)
    dbuf[...] = mm(low[:, :LEN], up[0]).astype(bf16)
    rbuf[...] = mm(low[:, LEN:], up[1]).astype(bf16)

    def project(weight, to, count):
        def body(i, carry):
            at = pl.ds(pl.multiple_of(i * 256, 256), 256)
            to[:, at] = mm(normed[0:count], weight[:, at]).astype(bf16)
            return carry

        lax.fori_loop(0, width // 256, body, 0)

    phase("proj_kv")
    copies[13].wait()
    project(wk, kbuf, LEN + ctx_n)
    copies[14].wait()
    project(wv, vbuf, LEN + ctx_n)

    phase("ctx_pack")
    lane = lax.broadcasted_iota(jnp.int32, (1, LEN), 1)
    left = lane < HALF
    for p in range(width // LEN):
        cols = slice(p * LEN, (p + 1) * LEN)
        for at, (first, second) in enumerate(((kbuf, vbuf), (dbuf, rbuf))):
            a = first[LEN : LEN + ctx_n, cols].astype(f32)
            b = second[LEN : LEN + ctx_n, cols].astype(f32)
            lanes = slice(at * LEN, (at + 1) * LEN)
            ctx_out[2 * p, :, lanes] = jnp.where(left, a, pltpu.roll(b, HALF, 1)).astype(bf16)
            ctx_out[2 * p + 1, :, lanes] = jnp.where(left, pltpu.roll(a, HALF, 1), b).astype(bf16)
        a = bias[0:1, cols]
        b = bias[1:2, cols]
        head_rows[2 * p : 2 * p + 1] = jnp.where(left, a, pltpu.roll(b, HALF, 1))
        head_rows[2 * p + 1 : 2 * p + 2] = jnp.where(left, pltpu.roll(a, HALF, 1), b)
    my_head = sp % 8
    backward = sp // 8
    ctx_in[sp] = ctx_out[my_head]

    for dz, dy in FAR_FIRST:
        to = at_offset(dz, dy)
        start(
            remote(
                ctx_out.at[to % 8], ctx_in.at[sp], c_s.at[4 * dz + dy], c_r.at[sp], to, tp
            )
        )

    phase("chunks")
    def place(to):
        slot = jnp.where(to == sp, N_SP, sp)
        return slot, jnp.where(to == sp, sibling, tp)

    def chunk():
        inputs = []
        for k in range(width // LEN):
            p = k
            cols = slice(p * LEN, (p + 1) * LEN)
            gates = jax.nn.sigmoid(bias[0:1, cols] + dbuf[0:LEN, cols].astype(f32))
            rate = jax.nn.sigmoid(bias[1:2, cols] + rbuf[0:LEN, cols].astype(f32))
            inputs.append(
                (
                    kbuf[0:LEN, cols].astype(f32),
                    vbuf[0:LEN, cols].astype(f32),
                    -DECAY_TOP * gates,
                    rate,
                )
            )

        def keep(p, rights, factors, scale):
            for direction in (0, 1):
                right_buf[p, direction] = rights[direction]
                factor_buf[p, direction] = factors[direction]
            scale_buf[p] = scale

        found = pairs_terms(inputs, keep)
        for p, (maps, solved) in enumerate(found):
            for direction in (0, 1):
                for head in (0, 1):
                    map_out[direction * 8 + 2 * p + head] = maps[2 * direction + head].astype(bf16)
        for dz, dy in FAR_FIRST:
            to = at_offset(dz, dy)
            start(remote(map_out.at[to], map_in.at[sp], m_s.at[to], m_r.at[sp], to, tp))
        for p, (maps, solved) in enumerate(found):
            for i in range(4):
                solved_buf[p, i] = solved[i]

    chunk()
    map_in[sp] = map_out[sp]

    phase("proj_qb")
    copies[15].wait()
    project(wq, qbuf, LEN)
    copies[16].wait()
    project(wb, bbuf, LEN)

    for j in (1, 2, 3):
        frm = (zz + j) % 4
        remote(gpart, gbuf.at[1, frm], gs_s.at[1, j], gs_r.at[1, frm], sp, tp).wait_recv()
    gmods[tp] = gbuf[1, 0] + gbuf[1, 1] + gbuf[1, 2] + gbuf[1, 3]
    for j in range(1, N_TP):
        to = (tp + j) % N_TP
        start(remote(gmods.at[tp], gmods.at[tp], gt_s.at[j], gt_r.at[tp], sp, to))

    phase("wait_ctx")
    for j in range(1, N_SP):
        frm = (sp + j) % N_SP
        remote(ctx_out.at[0], ctx_in.at[frm], c_s.at[j], c_r.at[frm], sp, tp).wait_recv()
    phase("ctx_chunks")
    my_bias = head_rows[pl.ds(my_head, 1)]
    per = LEN // ctx_n
    pairs, lows_in = [], []
    for c in range(N_SP // per):
        pairs.append(ctx_in[c * per : (c + 1) * per, :, 0:LEN].astype(f32).reshape(LEN, LEN))
        lows_in.append(ctx_in[c * per : (c + 1) * per, :, LEN:].astype(f32).reshape(LEN, LEN))
    for c, found in enumerate(context_terms(pairs, lows_in, my_bias, backward)):
        ctx_maps[c] = found
    count = N_SP // per
    forward = backward == 0
    order = [jnp.where(forward, i, N_SP - 1 - i) for i in range(N_SP)]
    state = ctx_maps[jnp.where(forward, 0, count - 1)]
    for c in range(1, count):
        state = compose(state, ctx_maps[jnp.where(forward, c, count - 1 - c)])
    left = lax.broadcasted_iota(jnp.int32, (1, LEN), 1) < HALF

    def show(i, state):
        state_out[order[i]] = jnp.where(
            left, pltpu.roll(state[: HALF // 2], HALF, 1), state[HALF // 2 :]
        ).astype(bf16)

    def launch(to):
        slot, over = place(to)
        remote(state_out.at[to], states.at[slot], s_s.at[to], s_r.at[slot], to, over).start()

    show(0, state)
    launch(order[0])
    ctx_state[...] = state

    phase("wait_maps")
    for copy in sends:
        copy.wait_send()
    drained = len(sends)
    for j in range(1, N_SP):
        frm = (sp + j) % N_SP
        remote(map_out.at[0], map_in.at[frm], m_s.at[0], m_r.at[frm], sp, tp).wait_recv()
    phase("walk")
    held = [ctx_state[...]] + [map_in[order[i]].astype(f32) for i in range(N_SP - 1)]
    size = 1
    while size < N_SP:
        held = [
            compose(held[i // size * size - 1], h) if i & size else h for i, h in enumerate(held)
        ]
        for i in range(size, 2 * size):
            show(i, held[i])
        if size < N_SP // 2:
            for i in range(size, 2 * size):
                launch(order[i])
        size *= 2
    base = jnp.where(forward, 2, 0)
    for dy in (2, 1, 3, 0):
        for k in (0, 1):
            launch((base + (zz + k) % 2) * 4 + (yy + dy) % 4)
    states[sp] = state_out[sp]

    phase("read_terms")

    def read_terms(p, carry):
        cols = pl.ds(pl.multiple_of(p * LEN, LEN), LEN)
        coming, here = pair_reads(
            qbuf[:, cols].astype(f32),
            vbuf[0:LEN, cols].astype(f32),
            [solved_buf[p, i] for i in range(4)],
            [right_buf[p, i] for i in range(2)],
            [factor_buf[p, i] for i in range(2)],
            scale_buf[p],
        )
        ahead[p] = coming.astype(bf16)
        local[p] = here
        return carry

    lax.fori_loop(0, width // LEN, read_terms, 0)

    phase("wait_states")
    for j in range(1, N_SP + 1):
        frm = (sp + j) % N_SP if j < N_SP else N_SP
        remote(state_out.at[0], states.at[frm], s_s.at[0], s_r.at[frm], sp, tp).wait_recv()

    phase("reads")
    for j in range(1, N_TP):
        frm = (tp + j) % N_TP
        remote(gpart, gmods.at[frm], gt_s.at[j], gt_r.at[frm], sp, tp).wait_recv()
    copies[17].wait()
    other = lane >= HALF
    for p in range(width // LEN):
        cols = slice(p * LEN, (p + 1) * LEN)
        blocks_in = []
        for at in (2 * p, 8 + 2 * p):
            first, second = states[at].astype(f32), states[at + 1].astype(f32)
            blocks_in += [
                jnp.where(left, first, 0.0),
                jnp.where(left, pltpu.roll(first, HALF, 1), 0.0),
                jnp.where(left, 0.0, pltpu.roll(second, HALF, 1)),
                jnp.where(left, 0.0, second),
            ]
        both = jnp.concatenate(blocks_in, axis=0).astype(bf16)
        reads = mm(ahead[p], both) + local[p]

        def head_mean(x):
            sums = [
                jnp.sum(jnp.where(mask, x, 0.0), axis=-1, keepdims=True) for mask in (left, other)
            ]
            return jnp.where(left, sums[0], sums[1]) * (1.0 / HALF)

        centred = reads - head_mean(reads)
        normal = centred * lax.rsqrt(head_mean(centred * centred) + GROUP_EPS)
        gate = bbuf[:, cols].astype(f32)
        mixed[:, cols] = (
            normal * ggain[0:1, cols] * (gate * jax.nn.sigmoid(gate))
        ).astype(bf16)

    phase("out_proj")
    copies[18].wait()
    n_chunk = arrived.shape[0]
    piece = model // n_chunk

    def chip_sum(c, x):
        return partial[c, core, x].astype(f32) + paired[c, x].astype(f32)

    def send_x(c, j):
        x = (xx + j) % 4
        start(
            remote(
                summed.at[c, j - 1], arrived.at[c, j - 1], g_s.at[c, j - 1], g_r.at[c, j - 1], sp,
                2 * x + core,
            )
        )

    def pass_on(c):
        remote(partial.at[c, 0], paired.at[c], o_s.at[c], o_r.at[c], sp, tp).wait_recv()
        for j in (2, 1, 3):
            summed[c, j - 1] = chip_sum(c, (xx + j) % 4).astype(bf16)
        send_x(c, 2)
        if c % 2 == 1:
            for at in (c - 1, c):
                send_x(at, 1)
                send_x(at, 3)

    for c in range(n_chunk):
        cols = slice(c * piece, (c + 1) * piece)
        product = mm(mixed[...], wo[:, cols]).astype(bf16)
        for x in range(4):
            for k in range(2):
                lo = (2 * x + k) * own_n
                partial[c, k, x] = product[lo : lo + own_n]
        start(
            remote(
                partial.at[c, 1 - core], paired.at[c], o_s.at[c], o_r.at[c], sp, sibling
            )
        )
        if c >= lag:
            pass_on(c - lag)
    phase("wait_core")
    for c in range(n_chunk - lag, n_chunk):
        pass_on(c)
    phase("wait_x")
    pieces = []
    for c in range(n_chunk):
        for k in (0, 2, 1):
            remote(
                summed.at[c, 0], arrived.at[c, k], g_s.at[c, k], g_r.at[c, k], sp, tp
            ).wait_recv()
        total = chip_sum(c, xx)
        for k in range(3):
            total = total + arrived[c, k].astype(f32)
        pieces.append(total.astype(bf16).astype(f32))
    phase("final")
    square = sum(jnp.sum(p * p, axis=-1, keepdims=True) for p in pieces)
    inverse = lax.rsqrt(square * (1.0 / model) + NORM_EPS)
    for c in range(n_chunk):
        for k in range(piece // LEN):
            lo = c * piece + k * LEN
            cols = slice(lo, lo + LEN)
            lane_block = lo // LEN
            per_tp = width // LEN
            gate = gmods[lane_block // per_tp, lane_block % per_tp : lane_block % per_tp + 1]
            value = pieces[c][:, k * LEN : (k + 1) * LEN]
            result[:, cols] = (own_rows[:, cols].astype(f32) + gate * (value * inverse)).astype(bf16)

    phase("drain")
    put = pltpu.make_async_copy(result, out, load.at[0])
    put.start()
    for copy in sends[drained:]:
        copy.wait_send()

    for j in range(N_SP):
        remote(state_out.at[0], states.at[0], s_s.at[j], s_r.at[0], sp, tp).wait_send()
    put.wait()
    scopes.close()


def on_device(
    latent,
    context,
    condition,
    context_condition,
    shift_weight,
    scale_weight,
    gate_weight,
    norm_gain,
    decay_down,
    decay_up,
    rate_down,
    rate_up,
    head_bias,
    query_weight,
    key_weight,
    value_weight,
    branch_weight,
    group_gain,
    out_weight,
):
    own_n, model = latent.shape
    ctx_n = context.shape[0]
    width = query_weight.shape[1]
    held = condition.shape[0]
    args = (
        latent,
        context,
        condition.reshape(1, -1),
        context_condition.reshape(1, -1),
        shift_weight,
        scale_weight,
        gate_weight,
        norm_gain.reshape(1, -1),
        decay_down,
        decay_up,
        rate_down,
        rate_up,
        head_bias,
        query_weight,
        key_weight,
        value_weight,
        branch_weight,
        group_gain.reshape(1, -1),
        out_weight,
    )
    n_chunk = 8
    piece = model // n_chunk
    V = pltpu.VMEM
    dma = pltpu.SemaphoreType.DMA
    scratch = [
        V((own_n, model), bf16),
        V((N_TP, own_n, model), bf16),
        V((own_n, model), bf16),
        V((ctx_n, model), bf16),
        V((2, held), f32),
        V((3, held, width), bf16),
        V((1, model), f32),
        V((model, 2 * LEN), bf16),
        V((2, LEN, width), bf16),
        V((2, width), f32),
        V((model, width), bf16),
        V((model, width), bf16),
        V((model, width), bf16),
        V((model, width), bf16),
        V((1, width), f32),
        V((width, model), bf16),
        V((8, width // 2), f32),
        V((4, 8, width // 2), f32),
        V((8, width // 2), f32),
        V((4, 8, width // 2), f32),
        V((N_TP, 8, width // 2), f32),
        V((8, LEN), f32),
        V((2, 4, 8, LEN), f32),
        V((1, 8, LEN), f32),
        V((N_TP, 8, LEN), f32),
        V((LEN + ctx_n, model), bf16),
        V((LEN + ctx_n, 2 * LEN), bf16),
        V((LEN + ctx_n, width), bf16),
        V((LEN + ctx_n, width), bf16),
        V((LEN + ctx_n, width), bf16),
        V((LEN + ctx_n, width), bf16),
        V((LEN, width), bf16),
        V((LEN, width), bf16),
        V((8, ctx_n, 2 * LEN), bf16),
        V((N_SP, ctx_n, 2 * LEN), bf16),
        V((8, LEN), f32),
        V((N_SP, HALF, LEN), bf16),
        V((N_SP + 1, HALF, LEN), bf16),
        V((4, HALF, LEN), f32),
        V((HALF, LEN), f32),
        V((width // LEN, 4, LEN, LEN), bf16),
        V((width // LEN, 2, 2 * LEN, LEN), bf16),
        V((width // LEN, 2, LEN, LEN), f32),
        V((width // LEN, 1, LEN), f32),
        V((width // LEN, LEN, 2 * LEN), bf16),
        V((width // LEN, LEN, LEN), f32),
        V((N_SP, HALF // 2, LEN), bf16),
        V((N_SP + 1, HALF // 2, LEN), bf16),
        V((LEN, width), bf16),
        V((n_chunk, 2, 4, own_n, piece), bf16),
        V((n_chunk, 4, own_n, piece), bf16),
        V((n_chunk, 3, own_n, piece), bf16),
        V((n_chunk, 3, own_n, piece), bf16),
        dma((19,)),
        dma((4,)),
        dma((4,)),
        dma((4,)),
        dma((4,)),
        dma((N_TP,)),
        dma((N_TP,)),
        dma((4,)),
        dma((N_TP,)),
        dma((4,)),
        dma((N_SP,)),
        dma((N_SP,)),
        dma((N_SP,)),
        dma((N_SP + 1,)),
        dma((N_SP,)),
        dma((N_SP + 1,)),
        dma((n_chunk,)),
        dma((n_chunk,)),
        dma((n_chunk, 3)),
        dma((n_chunk, 3)),
        dma((2, 4)),
        dma((2, 4)),
        dma((N_TP,)),
        dma((N_TP,)),
    ]
    return pl.pallas_call(
        kernel,
        out_shape=jax.ShapeDtypeStruct((own_n, model), bf16),
        in_specs=[pl.BlockSpec(memory_space=pltpu.HBM)] * len(args),
        out_specs=pl.BlockSpec(memory_space=pl.ANY),
        scratch_shapes=scratch,
        compiler_params=pltpu.CompilerParams(
            collective_id=0, has_side_effects=True, vmem_limit_bytes=44 * 1024 * 1024
        ),
    )(*(pltpu.with_memory_space_constraint(a, pltpu.HBM) for a in args))


def solution(mesh):
    placed = (
        P(("sp", "tp"), None),
        P("sp", None),
        P("sp"),
        P("sp"),
        P("sp", "tp"),
        P("sp", "tp"),
        P("sp", "tp"),
        P(),
        P(),
        P(None, "tp"),
        P(),
        P(None, "tp"),
        P(None, "tp"),
        P(None, "tp"),
        P(None, "tp"),
        P(None, "tp"),
        P(None, "tp"),
        P("tp"),
        P("tp", None),
    )
    return jax.shard_map(
        on_device, mesh=mesh, in_specs=placed, out_specs=P(("sp", "tp"), None), check_vma=False
    )
```
